256 devices in a mesh: gr: 2 (over z_hi), fs: 16 (over z_lo, x), tp: 8 (over y, core).
Axes of the slice: x: 4, y: 4, z: 8 (z_hi: 2, z_lo: 4; z = z_hi * 4 + z_lo), core: 2. Of those that a mesh axis runs over, the one named last changes fastest.
Arguments:
- tokens: bfloat16 [32768, 2048], P(('gr', 'fs', 'tp')), may hold values from -6 to 6
- norm_gain: float32 [2048], P('fs'), may hold values from 0.1 to 1.9
- gate_master: float32 [128, 2048, 256], P(None, 'fs', ('gr', 'tp')), may hold values from -0.125 to 0.125
- up_master: float32 [128, 2048, 256], P(None, 'fs', ('gr', 'tp')), may hold values from -0.125 to 0.125
- down_master: float32 [128, 256, 2048], P(None, 'fs', ('gr', 'tp')), may hold values from -0.375 to 0.375
- route_group: int32 [32768], P(('gr', 'fs', 'tp')), may hold values from 0 to 3
- route_expert: int32 [32768, 2], P(('gr', 'fs', 'tp')), may hold values from 0 to 31, all different within a row
- route_weight: float32 [32768, 2], P(('gr', 'fs', 'tp')), may hold values from 0.1 to 1
Outputs:
- gate_new: bfloat16 [128, 2048, 256], P(('fs', 'tp'))
- up_new: bfloat16 [128, 2048, 256], P(('fs', 'tp'))
- down_new: bfloat16 [128, 256, 2048], P(('fs', 'tp'))
- mixed: bfloat16 [32768, 2048], P(('gr', 'fs', 'tp'))
The draws below stay inside these ranges and needn't reach their ends.
Inputs may be any that keep to these rules, and one draw needn't show every extreme that they name: `route_expert`: the 2 entries of a row are different.
All inputs are finite; a program needn't handle non-finite values.
Results may differ from the reference program's by a relative error of at most 0.0086.
Values may be sent and summed in bfloat16 or wider, within the bound.
A program may use at most 64 MiB of HBM per device.

```python
import math
import jax
import jax.numpy as jnp
from jax import lax

D = 2048
F = 256
E_GROUPS = 4
TOP = 2
TOK_DEV = 128
EXPERTS = 128
EPG = 32
TOKENS = 32768
CAP = 3


def touch_ends(drawn, stream_key, smallest, top_value):
    place = [jax.random.randint(jax.random.fold_in(stream_key, axis), (), 0, length) for axis, length in enumerate(drawn.shape)]
    longest = drawn.shape.index(max(drawn.shape))
    next_to = place[:longest] + [(place[longest] + 1) % drawn.shape[longest]] + place[longest + 1:]
    return drawn.at[tuple(place)].set(smallest).at[tuple(next_to)].set(top_value)


def steps_of(rng, dims, cuts, low, high):
    loudness, own = 1.0, jax.random.fold_in(rng, 6)
    for dim, blocks in cuts:
        steps = jnp.exp(jax.random.uniform(jax.random.fold_in(own, dim), (blocks,), jnp.float32, low / len(cuts), high / len(cuts)))
        loudness = loudness * jnp.repeat(steps, dims[dim] // blocks).reshape([-1 if axis == dim else 1 for axis in range(len(dims))])
    return loudness


def choose_distinct(key, rows, number_of, top, lift):
    order = jax.random.permutation(jax.random.fold_in(key, 1), number_of)
    pull = order
    for power in range(3):
        pull = pull * pull // number_of
    pull = pull * lift // number_of
    tickets = jax.random.randint(jax.random.fold_in(key, 2), (rows, number_of), 0, 4096) + pull
    fixed_rows = jax.random.permutation(jax.random.fold_in(key, 3), rows)[jnp.arange(number_of) % rows]
    tickets = jnp.where(jnp.arange(rows)[:, None] == fixed_rows[None, :], 1 << 14, tickets)
    priority = tickets * number_of + jnp.arange(number_of)
    return lax.top_k(priority.astype(jnp.int32), top)[1].astype(jnp.int32)


def scatter_about(key, shape, scale, most, shards=(), held_as=jnp.bfloat16):
    gain = steps_of(key, shape, shards, -0.22, 0.18) if shards else 1.0
    result = jax.random.normal(key, shape, jnp.float32) * scale * gain
    return jnp.minimum(jnp.maximum(result, -most), most).astype(held_as)


def setup_inputs(seed: int = 0) -> dict:
    seeds = jax.random.split(jax.random.key(seed), 9)
    return {
        "tokens": scatter_about(seeds[0], (TOKENS, D), 1.0, 6.0, ((0, 256),)),
        "norm_gain": jnp.clip(1.0 + 0.18 * jax.random.normal(seeds[1], (D,), jnp.float32), 0.1, 1.9),
        "gate_master": scatter_about(seeds[2], (EXPERTS, D, F), D ** -0.5, 0.125, ((1, 16), (2, 16)), jnp.float32),
        "up_master": scatter_about(seeds[3], (EXPERTS, D, F), D ** -0.5, 0.125, ((1, 16), (2, 16)), jnp.float32),
        "down_master": scatter_about(seeds[4], (EXPERTS, F, D), F ** -0.5, 0.375, ((1, 16), (2, 16)), jnp.float32),
        "route_group": touch_ends(jax.random.randint(seeds[5], (TOKENS,), 0, E_GROUPS), jax.random.fold_in(seeds[5], 1), 0, E_GROUPS - 1).astype(jnp.int32),
        "route_expert": choose_distinct(seeds[6], TOKENS, EPG, TOP, 512),
        "route_weight": jnp.clip(jnp.exp(math.log(1.0) - 2.3025851 * jax.random.uniform(seeds[7], (TOKENS, TOP), jnp.float32) ** steps_of(seeds[7], (TOKENS, TOP), ((0, 256),), -0.2, 0.2)), 0.1, 1.0),
    }


def reference(tokens, norm_gain, gate_master, up_master, down_master, route_group, route_expert, route_weight):
    gate_new = (gate_master * norm_gain[None, :, None]).astype(jnp.bfloat16)
    up_new = (up_master * norm_gain[None, :, None]).astype(jnp.bfloat16)
    down_new = down_master.astype(jnp.bfloat16)
    floats = tokens.astype(jnp.float32)
    normed = (floats * lax.rsqrt(lax.optimization_barrier(jnp.mean(floats * floats, axis=-1, keepdims=True)) + 1e-06)).astype(jnp.bfloat16)
    sources = TOKENS // TOK_DEV
    expert_id = (route_group[:, None] * EPG + route_expert).astype(jnp.int32)
    blocks = expert_id.reshape(sources, TOK_DEV * TOP)
    columns = jnp.arange(EXPERTS).astype(jnp.int32)
    onehot = (blocks[:, :, None] == columns[None, None, :]).astype(jnp.int32)
    rank = lax.optimization_barrier(jnp.sum((jnp.cumsum(onehot, axis=1) - 1) * onehot, axis=2)).astype(jnp.int32)
    source_ids = jnp.arange(sources).astype(jnp.int32)[:, None]
    dump = EXPERTS * sources * CAP
    slot = jnp.where(rank < CAP, blocks * (sources * CAP) + source_ids * CAP + rank, dump).reshape(-1).astype(jnp.int32)
    rows = jnp.repeat(normed, TOP, axis=0)
    buffer = jnp.zeros((dump + 1, D), jnp.bfloat16).at[slot].set(rows)[:-1].reshape(EXPERTS, sources * CAP, D)

    def expert(operands):
        block, w_gate, w_up, w_down = operands
        gate = jnp.dot(block, w_gate, preferred_element_type=jnp.float32)
        upper = jnp.dot(block, w_up, preferred_element_type=jnp.float32)
        hidden = (jax.nn.silu(gate) * upper).astype(jnp.bfloat16)
        return jnp.dot(hidden, w_down, preferred_element_type=jnp.float32).astype(jnp.bfloat16)
    outcome = lax.map(expert, (buffer, gate_new, up_new, down_new))
    table = jnp.concatenate([outcome.reshape(-1, D), jnp.zeros((1, D), jnp.bfloat16)], axis=0)
    picked = table[slot].reshape(TOKENS, TOP, D).astype(jnp.float32)
    mixed = lax.optimization_barrier(jnp.sum(picked * route_weight[:, :, None], axis=1)).astype(jnp.bfloat16)
    return (gate_new, up_new, down_new, mixed)
```

```python
import functools

import jax
import jax.numpy as jnp
from jax import lax
from jax.experimental import pallas as pl
from jax.experimental.pallas import tpu as pltpu
from jax.sharding import PartitionSpec as P

MESH = pl.DeviceIdType.MESH
BF16 = jnp.bfloat16
F32 = jnp.float32

PLANES, GROUPS, INPLANE = 8, 4, 32
TOK, D, F, CAP = 128, 2048, 256, 3
GROUP_ROWS = INPLANE * CAP
SLOTS = GROUPS * GROUP_ROWS
PAIR_ROWS = 16
EXP_ROWS = INPLANE * PAIR_ROWS
NCH = 4
COLS = D // NCH
FAR_FIRST = (4, 3, 5, 2, 6, 1, 7)


def nt_dot(a, b):
    return lax.dot_general(a, b, (((1,), (1,)), ((), ())), preferred_element_type=F32)


def mm(a, b):
    return jnp.dot(a, b, preferred_element_type=F32)


def kernel(
    gate_in, up_in, down_in, gain, tok_in, group, expert, weight,
    gate_out, up_out, down_out, mixed_out,
    fbuf, wgu, wd, zgu, zd, fgu, fd,
    tokv, xzs, xz, xp, xe, hid,
    gt, ut, dn, go, uo, r, rr, q, t, mix,
    in_sem, out_sem, send_z, send_p, rz_gu, rz_d, rz_t, rz_r, rp_gu, rp_d, rp_t, rp_r,
):
    gr, fs, tp = lax.axis_index("gr"), lax.axis_index("fs"), lax.axis_index("tp")
    zl, x = lax.div(fs, 4), lax.rem(fs, 4)
    y, c = lax.div(tp, 2), lax.rem(tp, 2)
    z = gr * 4 + zl
    me = x * 8 + tp

    def z_device(target):
        return (lax.div(target, 4), lax.rem(target, 4) * 4 + x, tp)

    def hop(j):
        o = lax.rem(j * 11, INPLANE)
        tx = lax.rem(x + lax.div(o, 8), 4)
        ty = lax.rem(y + lax.rem(lax.div(o, 2), 4), 4)
        ttp = ty * 2 + lax.rem(c + lax.rem(o, 2), 2)
        return tx * 8 + ttp, (gr, zl * 4 + tx, ttp)

    def remote(src, dst, send, recv, device):
        pltpu.make_async_remote_copy(
            src_ref=src, dst_ref=dst, send_sem=send, recv_sem=recv, device_id=device, device_id_type=MESH
        ).start()

    def wait_bytes(ref, sem):
        pltpu.make_async_copy(ref, ref, sem).wait()

    barrier = pltpu.get_barrier_semaphore()
    for d in FAR_FIRST:
        pl.semaphore_signal(barrier, inc=1, device_id=z_device(lax.rem(z + d, PLANES)), device_id_type=MESH)

    @pl.loop(1, INPLANE)
    def _(j):
        pl.semaphore_signal(barrier, inc=1, device_id=hop(j)[1], device_id_type=MESH)

    inputs = [
        pltpu.make_async_copy(src, dst, in_sem.at[i])
        for i, (src, dst) in enumerate(
            ((gate_in, fbuf.at[0]), (up_in, fbuf.at[1]), (down_in, fbuf.at[2]), (tok_in, tokv))
        )
    ]
    for copy in inputs:
        copy.start()
    inputs[0].wait()
    inputs[1].wait()
    scale = gain[...].reshape(1, 1, 128)

    @pl.loop(0, 16)
    def _(i):
        e = pl.ds(i * 8, 8)
        wgu[e, 0:16, :] = (fbuf[0, e] * scale).astype(BF16)
        wgu[e, 16:32, :] = (fbuf[1, e] * scale).astype(BF16)

    inputs[2].wait()

    @pl.loop(0, 16)
    def _(i):
        e = pl.ds(i * 8, 8)
        wd[e] = fbuf[2, e].astype(BF16)

    pl.semaphore_wait(barrier, len(FAR_FIRST) + INPLANE - 1)

    def send_planes(src, dst, recv):
        for d in FAR_FIRST:
            target = lax.rem(z + d, PLANES)
            experts = pl.ds(lax.rem(target, 4) * INPLANE, INPLANE)
            remote(src.at[experts], dst.at[z], send_z, recv.at[z], z_device(target))

    def forward(src, base, dst, plane, recv):
        @pl.loop(1, INPLANE)
        def _(j):
            place, device = hop(j)
            remote(src.at[base + place], dst.at[plane, me], send_p, recv, device)

    send_planes(wgu, zgu, rz_gu)
    forward(wgu, zl * INPLANE, fgu, z, rp_gu)
    fgu[z, me] = wgu[zl * INPLANE + me]
    fd[z, me] = wd[zl * INPLANE + me]

    inputs[3].wait()

    @pl.loop(0, 4)
    def _(i):
        rows = pl.ds(i * 32, 32)
        v = tokv[rows, :].astype(F32)
        v = v * lax.rsqrt(jnp.mean(v * v, axis=-1, keepdims=True) + 1e-06)
        tokv[rows, :] = v.astype(BF16)

    ids = group[...] * INPLANE + expert[...]
    expert_iota = lax.broadcasted_iota(jnp.int32, (128, TOK), 0)
    one = [(expert_iota == ids[k : k + 1, :]).astype(F32) for k in range(2)]
    lane_iota = lax.broadcasted_iota(jnp.int32, (128, TOK), 1)
    earlier = (expert_iota < lane_iota).astype(BF16)
    count = mm((one[0] + one[1]).astype(BF16), earlier)
    slot_iota = lax.broadcasted_iota(jnp.int32, (SLOTS, TOK), 0)
    pick = []
    for k in range(2):
        rank = jnp.sum(one[k] * count, axis=0, keepdims=True).astype(jnp.int32)
        slot = jnp.where(rank < CAP, ids[k : k + 1, :] * CAP + rank, -1)
        pick.append((slot_iota == slot).astype(F32))
    rows_of = (pick[0] + pick[1]).astype(BF16)
    for n in range(NCH):
        cols = slice(n * COLS, (n + 1) * COLS)
        xzs[:, :, cols] = mm(rows_of, tokv[:, cols]).astype(BF16).reshape(GROUPS, GROUP_ROWS, COLS)
    for d in (3, 2, 1):
        for target, there in ((zl + d, zl + d < GROUPS), (zl - d, zl - d >= 0)):

            @pl.when(there)
            def _(target=target):
                remote(xzs.at[target], xz.at[zl], send_z, rz_t, (gr, target * 4 + x, tp))

    send_planes(wd, zd, rz_d)
    forward(wd, zl * INPLANE, fd, z, rp_d)

    @pl.loop(0, GROUP_ROWS // 16)
    def _(i):
        rows = pl.ds(i * 16, 16)
        xz[zl, rows, :] = xzs[zl, rows, :]

    def relay(d, src, dst, rz, rp):
        plane = lax.rem(z + PLANES - d, PLANES)
        wait_bytes(src.at[plane], rz.at[plane])

        @pl.loop(1, INPLANE)
        def _(j):
            place, device = hop(j)
            remote(src.at[plane, place], dst.at[plane, me], send_p, rp, device)

        dst[plane, me] = src[plane, me]

    for d in FAR_FIRST:
        relay(d, zgu, fgu, rz_gu, rp_gu)

    def placed(i):
        within = i % PAIR_ROWS
        plane = (within >= 3).astype(jnp.int32) + (within >= 6).astype(jnp.int32) + (within >= 9).astype(jnp.int32)
        at = plane * GROUP_ROWS + (i // PAIR_ROWS) * CAP + within - plane * CAP
        return jnp.where(within < GROUPS * CAP, at, -1)

    wait_bytes(xz.at[pl.ds(0, GROUPS - 1)], rz_t)
    order = (
        placed(lax.broadcasted_iota(jnp.int32, (EXP_ROWS, SLOTS), 0))
        == lax.broadcasted_iota(jnp.int32, (EXP_ROWS, SLOTS), 1)
    ).astype(F32).astype(BF16)
    for n in range(NCH):
        cols = slice(n * COLS, (n + 1) * COLS)
        moved = mm(order, xz[:, :, cols].reshape(SLOTS, COLS))
        xp[:, :, cols] = moved.astype(BF16).reshape(INPLANE, PAIR_ROWS, COLS)

    @pl.loop(1, INPLANE)
    def _(j):
        place, device = hop(j)
        remote(xp.at[place], xe.at[me], send_p, rp_t, device)

    xe[me] = xp[me]

    for d in FAR_FIRST[:4]:
        relay(d, zd, fd, rz_d, rp_d)

    wait_bytes(fgu.at[:, pl.ds(0, INPLANE - 1)], rp_gu)
    for h in range(2):
        for s in range(4):
            for px in range(4):
                rows, cols = slice(h * 128, (h + 1) * 128), slice((s * 4 + px) * 128, (s * 4 + px + 1) * 128)
                tiles = slice(px * 8, (px + 1) * 8)
                gt[rows, cols] = fgu[h * 4 + s, tiles, 0:16, :].reshape(128, 128)
                ut[rows, cols] = fgu[h * 4 + s, tiles, 16:32, :].reshape(128, 128)
    wait_bytes(xe.at[pl.ds(0, INPLANE - 1)], rp_t)

    @pl.loop(0, EXP_ROWS // 128)
    def _(i):
        rows = xe[pl.ds(i * 8, 8)].reshape(128, D)
        gate = nt_dot(rows, gt[...])
        upper = nt_dot(rows, ut[...])
        hid[pl.ds(i * 128, 128), :] = (gate / (1.0 + jnp.exp(-gate)) * upper).astype(BF16)

    for d in FAR_FIRST[4:]:
        relay(d, zd, fd, rz_d, rp_d)

    wait_bytes(fd.at[:, pl.ds(0, INPLANE - 1)], rp_d)
    for h in range(2):
        for s in range(4):
            for px in range(4):
                for place in range(8):
                    col = h * 8 + place
                    dn[(s * 4 + px) * 16 : (s * 4 + px + 1) * 16, col * 128 : (col + 1) * 128] = fd[
                        h * 4 + s, px * 8 + place
                    ]
    for n in range(NCH):
        cols = slice(n * COLS, (n + 1) * COLS)
        result = mm(hid[...], dn[:, cols])
        r[n] = result.astype(BF16).reshape(INPLANE, PAIR_ROWS, COLS)

        @pl.loop(1, INPLANE)
        def _(j):
            place, device = hop(j)
            remote(r.at[n, place], rr.at[n, me], send_p, rp_r.at[n], device)

        rr[n, me] = r[n, me]

    back = (
        placed(lax.broadcasted_iota(jnp.int32, (SLOTS, EXP_ROWS), 1))
        == lax.broadcasted_iota(jnp.int32, (SLOTS, EXP_ROWS), 0)
    ).astype(F32).astype(BF16)
    for n in range(NCH):
        wait_bytes(rr.at[n, pl.ds(0, INPLANE - 1)], rp_r.at[n])
        moved = mm(back, rr[n].reshape(EXP_ROWS, COLS))
        q[n] = moved.astype(BF16).reshape(GROUPS, GROUP_ROWS, COLS)
        for d in (3, 2, 1):
            for target, there in ((zl + d, zl + d < GROUPS), (zl - d, zl - d >= 0)):

                @pl.when(there)
                def _(target=target):
                    remote(q.at[n, target], t.at[n, zl], send_z, rz_r.at[n], (gr, target * 4 + x, tp))

        t[n, zl] = q[n, zl]

    down_copy = pltpu.make_async_copy(dn, down_out.at[0], out_sem.at[2])
    down_copy.start()
    for h in range(2):
        for s in range(16):
            rows, cols = slice(h * 128, (h + 1) * 128), slice(s * 128, (s + 1) * 128)
            go[cols, rows] = gt[rows, cols].T
            uo[cols, rows] = ut[rows, cols].T
    gate_copy = pltpu.make_async_copy(go, gate_out.at[0], out_sem.at[0])
    up_copy = pltpu.make_async_copy(uo, up_out.at[0], out_sem.at[1])
    gate_copy.start()
    up_copy.start()

    select = [p.T.astype(BF16) for p in pick]
    weights = [jnp.broadcast_to(weight[k : k + 1, :], (128, TOK)).T[:, 0:1] for k in range(2)]
    for n in range(NCH):
        cols = slice(n * COLS, (n + 1) * COLS)
        wait_bytes(t.at[n, pl.ds(0, GROUPS - 1)], rz_r.at[n])
        table = t[n].reshape(SLOTS, COLS)
        mix[:, cols] = (mm(select[0], table) * weights[0] + mm(select[1], table) * weights[1]).astype(BF16)
    mixed_copy = pltpu.make_async_copy(mix, mixed_out, out_sem.at[3])
    mixed_copy.start()

    others = pl.ds(0, PLANES - 1)
    wait_bytes(zgu.at[others], send_z)
    wait_bytes(zd.at[others], send_z)
    wait_bytes(xz.at[pl.ds(0, GROUPS - 1)], send_z)
    wait_bytes(fgu.at[:, pl.ds(0, INPLANE - 1)], send_p)
    wait_bytes(fd.at[:, pl.ds(0, INPLANE - 1)], send_p)
    wait_bytes(xe.at[pl.ds(0, INPLANE - 1)], send_p)
    for n in range(NCH):
        wait_bytes(t.at[n, pl.ds(0, GROUPS - 1)], send_z)
        wait_bytes(rr.at[n, pl.ds(0, INPLANE - 1)], send_p)
    down_copy.wait()
    gate_copy.wait()
    up_copy.wait()
    mixed_copy.wait()


def body(
    tokens, norm_gain, gate_master, up_master, down_master, route_group, route_expert, route_weight
):
    vmem, hbm = pl.BlockSpec(memory_space=pltpu.VMEM), pl.BlockSpec(memory_space=pl.ANY)
    dma = pltpu.SemaphoreType.DMA
    tile = pltpu.VMEM
    return pl.pallas_call(
        kernel,
        out_shape=(
            jax.ShapeDtypeStruct((1, D, F), BF16),
            jax.ShapeDtypeStruct((1, D, F), BF16),
            jax.ShapeDtypeStruct((1, F, D), BF16),
            jax.ShapeDtypeStruct((TOK, D), BF16),
        ),
        in_specs=[hbm, hbm, hbm, vmem, hbm, vmem, vmem, vmem],
        out_specs=(hbm, hbm, hbm, hbm),
        scratch_shapes=[
            tile((3, 128, 16, 128), F32),
            tile((128, 32, 128), BF16),
            tile((128, 16, 128), BF16),
            tile((PLANES, INPLANE, 32, 128), BF16),
            tile((PLANES, INPLANE, 16, 128), BF16),
            tile((PLANES, INPLANE, 32, 128), BF16),
            tile((PLANES, INPLANE, 16, 128), BF16),
            tile((TOK, D), BF16),
            tile((GROUPS, GROUP_ROWS, D), BF16),
            tile((GROUPS, GROUP_ROWS, D), BF16),
            tile((INPLANE, PAIR_ROWS, D), BF16),
            tile((INPLANE, PAIR_ROWS, D), BF16),
            tile((EXP_ROWS, F), BF16),
            tile((F, D), BF16),
            tile((F, D), BF16),
            tile((F, D), BF16),
            tile((D, F), BF16),
            tile((D, F), BF16),
            tile((NCH, INPLANE, PAIR_ROWS, COLS), BF16),
            tile((NCH, INPLANE, PAIR_ROWS, COLS), BF16),
            tile((NCH, GROUPS, GROUP_ROWS, COLS), BF16),
            tile((NCH, GROUPS, GROUP_ROWS, COLS), BF16),
            tile((TOK, D), BF16),
            dma((4,)),
            dma((4,)),
            dma,
            dma,
            dma((PLANES,)),
            dma((PLANES,)),
            dma,
            dma((NCH,)),
            dma,
            dma,
            dma,
            dma((NCH,)),
        ],
        compiler_params=pltpu.CompilerParams(
            collective_id=0, has_side_effects=True, vmem_limit_bytes=60 * 2**20
        ),
    )(
        jnp.swapaxes(gate_master, 1, 2),
        jnp.swapaxes(up_master, 1, 2),
        down_master,
        norm_gain[None],
        tokens,
        route_group[None],
        route_expert.T,
        route_weight.T,
    )


def solution(mesh):
    placed = (
        P(("gr", "fs", "tp"), None),
        P("fs"),
        P(None, "fs", ("gr", "tp")),
        P(None, "fs", ("gr", "tp")),
        P(None, "fs", ("gr", "tp")),
        P(("gr", "fs", "tp")),
        P(("gr", "fs", "tp"), None),
        P(("gr", "fs", "tp"), None),
    )
    return jax.shard_map(
        body,
        mesh=mesh,
        in_specs=placed,
        out_specs=(
            P(("fs", "tp"), None, None),
            P(("fs", "tp"), None, None),
            P(("fs", "tp"), None, None),
            P(("gr", "fs", "tp"), None),
        ),
        check_vma=False,
    )
```

```python
import functools

import jax
import jax.numpy as jnp
from jax import lax
from jax.experimental import pallas as pl
from jax.experimental.pallas import tpu as pltpu
from jax.sharding import PartitionSpec as P

MESH = pl.DeviceIdType.MESH
BF16 = jnp.bfloat16
F32 = jnp.float32

PLANES, GROUPS, INPLANE = 8, 4, 32
TOK, D, F, CAP = 128, 2048, 256, 3
GROUP_ROWS = INPLANE * CAP
SLOTS = GROUPS * GROUP_ROWS
PAIR_ROWS = 16
EXP_ROWS = INPLANE * PAIR_ROWS
NCH = 4
COLS = D // NCH
FAR_FIRST = (4, 3, 5, 2, 6, 1, 7)


def nt_dot(a, b):
    return lax.dot_general(a, b, (((1,), (1,)), ((), ())), preferred_element_type=F32)


def mm(a, b):
    return jnp.dot(a, b, preferred_element_type=F32)


def kernel(
    gate_in, up_in, down_in, gain, tok_in, group, expert, weight,
    gate_out, up_out, down_out, mixed_out,
    fbuf, wgu, wd, zgu, zd, fgu, fd,
    tokv, xzs, xz, xp, xe, hid,
    gt, ut, dn, go, uo, r, rr, q, t, mix,
    in_sem, out_sem, send_z, send_p, rz_gu, rz_d, rz_t, rz_r, rp_gu, rp_d, rp_t, rp_r,
):
    gr, fs, tp = lax.axis_index("gr"), lax.axis_index("fs"), lax.axis_index("tp")
    zl, x = lax.div(fs, 4), lax.rem(fs, 4)
    y, c = lax.div(tp, 2), lax.rem(tp, 2)
    z = gr * 4 + zl
    me = x * 8 + tp

    row_planes = [z] + [lax.rem(z + step, PLANES) for step in (1, 7, 2 + 4 * c)]
    row_sources = [z] + [lax.rem(z + step, PLANES) for step in (7, 1, 6 - 4 * c)]

    def z_device(target):
        return (lax.div(target, 4), lax.rem(target, 4) * 4 + x, tp)

    def hop(j):
        o = lax.rem(j * 11, INPLANE)
        tx = lax.rem(x + lax.div(o, 8), 4)
        ty = lax.rem(y + lax.rem(lax.div(o, 2), 4), 4)
        ttp = ty * 2 + lax.rem(c + lax.rem(o, 2), 2)
        return tx * 8 + ttp, (gr, zl * 4 + tx, ttp)

    def remote(src, dst, send, recv, device):
        pltpu.make_async_remote_copy(
            src_ref=src, dst_ref=dst, send_sem=send, recv_sem=recv, device_id=device, device_id_type=MESH
        ).start()

    def wait_bytes(ref, sem):
        pltpu.make_async_copy(ref, ref, sem).wait()

    barrier = pltpu.get_barrier_semaphore()
    for d in FAR_FIRST:
        pl.semaphore_signal(barrier, inc=1, device_id=z_device(lax.rem(z + d, PLANES)), device_id_type=MESH)

    @pl.loop(1, INPLANE)
    def _(j):
        pl.semaphore_signal(barrier, inc=1, device_id=hop(j)[1], device_id_type=MESH)

    inputs = [
        pltpu.make_async_copy(src, dst, in_sem.at[i])
        for i, (src, dst) in enumerate(
            ((gate_in, fbuf.at[0]), (up_in, fbuf.at[1]), (down_in, fbuf.at[2]), (tok_in, tokv))
        )
    ]
    for copy in inputs:
        copy.start()
    inputs[3].wait()

    @pl.loop(0, 4)
    def _(i):
        rows = pl.ds(i * 32, 32)
        v = tokv[rows, :].astype(F32)
        v = v * lax.rsqrt(jnp.mean(v * v, axis=-1, keepdims=True) + 1e-06)
        tokv[rows, :] = v.astype(BF16)

    ids = group[...] * INPLANE + expert[...]
    expert_iota = lax.broadcasted_iota(jnp.int32, (128, TOK), 0)
    one = [(expert_iota == ids[k : k + 1, :]).astype(F32) for k in range(2)]
    lane_iota = lax.broadcasted_iota(jnp.int32, (128, TOK), 1)
    earlier = (expert_iota < lane_iota).astype(BF16)
    count = mm((one[0] + one[1]).astype(BF16), earlier)
    slot_iota = lax.broadcasted_iota(jnp.int32, (SLOTS, TOK), 0)
    away = lax.rem(group[...] - zl + GROUPS, GROUPS)
    block = jnp.where(away == 2, 3, jnp.where(away == 3, 2, away))
    pick = []
    for k in range(2):
        rank = jnp.sum(one[k] * count, axis=0, keepdims=True).astype(jnp.int32)
        slot = jnp.where(rank < CAP, block * GROUP_ROWS + expert[k : k + 1, :] * CAP + rank, -1)
        pick.append((slot_iota == slot).astype(F32))
    rows_of = (pick[0] + pick[1]).astype(BF16)
    for n in range(NCH):
        cols = slice(n * COLS, (n + 1) * COLS)
        xzs[:, :, cols] = mm(rows_of, tokv[:, cols]).astype(BF16).reshape(GROUPS, GROUP_ROWS, COLS)
    inputs[0].wait()
    inputs[1].wait()
    scale = gain[...].reshape(1, 1, 128)

    @pl.loop(0, 16)
    def _(i):
        e = pl.ds(i * 8, 8)
        wgu[e, 0:16, :] = (fbuf[0, e] * scale).astype(BF16)
        wgu[e, 16:32, :] = (fbuf[1, e] * scale).astype(BF16)

    inputs[2].wait()

    @pl.loop(0, 16)
    def _(i):
        e = pl.ds(i * 8, 8)
        wd[e] = fbuf[2, e].astype(BF16)

    pl.semaphore_wait(barrier, len(FAR_FIRST) + INPLANE - 1)

    def send_planes(src, dst, recv, steps):
        for d in steps:
            target = lax.rem(z + d, PLANES)
            experts = pl.ds(lax.rem(target, 4) * INPLANE, INPLANE)
            remote(src.at[experts], dst.at[z], send_z, recv.at[z], z_device(target))

    def forward(src, base, dst, plane, recv):
        @pl.loop(1, INPLANE)
        def _(j):
            place, device = hop(j)
            remote(src.at[base + place], dst.at[plane, me], send_p, recv, device)

    for block in (3, 1, 2):
        remote(xzs.at[block], xz.at[block], send_z, rz_t, z_device(row_planes[block]))

    send_planes(wgu, zgu, rz_gu, FAR_FIRST)
    send_planes(wd, zd, rz_d, FAR_FIRST)
    forward(wgu, zl * INPLANE, fgu, z, rp_gu)
    forward(wd, zl * INPLANE, fd, z, rp_d)
    fgu[z, me] = wgu[zl * INPLANE + me]
    fd[z, me] = wd[zl * INPLANE + me]

    @pl.loop(0, GROUP_ROWS // 16)
    def _(i):
        rows = pl.ds(i * 16, 16)
        xz[0, rows, :] = xzs[0, rows, :]

    def relay(d, src, dst, rz, rp):
        plane = lax.rem(z + PLANES - d, PLANES)
        wait_bytes(src.at[plane], rz.at[plane])

        @pl.loop(1, INPLANE)
        def _(j):
            place, device = hop(j)
            remote(src.at[plane, place], dst.at[plane, me], send_p, rp, device)

        dst[plane, me] = src[plane, me]

    def placed(i):
        within = i % PAIR_ROWS
        block = (within >= 3).astype(jnp.int32) + (within >= 6).astype(jnp.int32) + (within >= 9).astype(jnp.int32)
        at = block * GROUP_ROWS + (i // PAIR_ROWS) * CAP + within - block * CAP
        return jnp.where(within < GROUPS * CAP, at, -1)

    wait_bytes(xz.at[pl.ds(1, GROUPS - 1)], rz_t)
    order = (
        placed(lax.broadcasted_iota(jnp.int32, (EXP_ROWS, SLOTS), 0))
        == lax.broadcasted_iota(jnp.int32, (EXP_ROWS, SLOTS), 1)
    ).astype(F32).astype(BF16)
    for n in range(NCH):
        cols = slice(n * COLS, (n + 1) * COLS)
        moved = mm(order, xz[:, :, cols].reshape(SLOTS, COLS))
        xp[:, :, cols] = moved.astype(BF16).reshape(INPLANE, PAIR_ROWS, COLS)

    @pl.loop(1, INPLANE)
    def _(j):
        place, device = hop(j)
        remote(xp.at[place], xe.at[me], send_p, rp_t, device)

    xe[me] = xp[me]

    for d in FAR_FIRST:
        relay(d, zgu, fgu, rz_gu, rp_gu)

    for d in FAR_FIRST[:4]:
        relay(d, zd, fd, rz_d, rp_d)

    wait_bytes(fgu.at[:, pl.ds(0, INPLANE - 1)], rp_gu)
    for h in range(2):
        for s in range(4):
            for px in range(4):
                rows, cols = slice(h * 128, (h + 1) * 128), slice((s * 4 + px) * 128, (s * 4 + px + 1) * 128)
                tiles = slice(px * 8, (px + 1) * 8)
                gt[rows, cols] = fgu[h * 4 + s, tiles, 0:16, :].reshape(128, 128)
                ut[rows, cols] = fgu[h * 4 + s, tiles, 16:32, :].reshape(128, 128)
    wait_bytes(xe.at[pl.ds(0, INPLANE - 1)], rp_t)

    @pl.loop(0, EXP_ROWS // 128)
    def _(i):
        rows = xe[pl.ds(i * 8, 8)].reshape(128, D)
        gate = nt_dot(rows, gt[...])
        upper = nt_dot(rows, ut[...])
        hid[pl.ds(i * 128, 128), :] = (gate / (1.0 + jnp.exp(-gate)) * upper).astype(BF16)

    for d in FAR_FIRST[4:]:
        relay(d, zd, fd, rz_d, rp_d)

    wait_bytes(fd.at[:, pl.ds(0, INPLANE - 1)], rp_d)
    for h in range(2):
        for s in range(4):
            for px in range(4):
                for place in range(8):
                    col = h * 8 + place
                    dn[(s * 4 + px) * 16 : (s * 4 + px + 1) * 16, col * 128 : (col + 1) * 128] = fd[
                        h * 4 + s, px * 8 + place
                    ]
    for n in range(NCH):
        cols = slice(n * COLS, (n + 1) * COLS)
        result = mm(hid[...], dn[:, cols])
        r[n] = result.astype(BF16).reshape(INPLANE, PAIR_ROWS, COLS)

        @pl.loop(1, INPLANE)
        def _(j):
            place, device = hop(j)
            remote(r.at[n, place], rr.at[n, me], send_p, rp_r.at[n], device)

        rr[n, me] = r[n, me]

    back = (
        placed(lax.broadcasted_iota(jnp.int32, (SLOTS, EXP_ROWS), 1))
        == lax.broadcasted_iota(jnp.int32, (SLOTS, EXP_ROWS), 0)
    ).astype(F32).astype(BF16)
    for n in range(NCH):
        wait_bytes(rr.at[n, pl.ds(0, INPLANE - 1)], rp_r.at[n])
        moved = mm(back, rr[n].reshape(EXP_ROWS, COLS))
        q[n] = moved.astype(BF16).reshape(GROUPS, GROUP_ROWS, COLS)
        for block in (3, 1, 2):
            remote(q.at[n, block], t.at[n, block], send_z, rz_r.at[n], z_device(row_sources[block]))

        t[n, 0] = q[n, 0]

    down_copy = pltpu.make_async_copy(dn, down_out.at[0], out_sem.at[2])
    down_copy.start()
    for h in range(2):
        for s in range(16):
            rows, cols = slice(h * 128, (h + 1) * 128), slice(s * 128, (s + 1) * 128)
            go[cols, rows] = gt[rows, cols].T
            uo[cols, rows] = ut[rows, cols].T
    gate_copy = pltpu.make_async_copy(go, gate_out.at[0], out_sem.at[0])
    up_copy = pltpu.make_async_copy(uo, up_out.at[0], out_sem.at[1])
    gate_copy.start()
    up_copy.start()

    select = [p.T.astype(BF16) for p in pick]
    weights = [jnp.broadcast_to(weight[k : k + 1, :], (128, TOK)).T[:, 0:1] for k in range(2)]
    for n in range(NCH):
        cols = slice(n * COLS, (n + 1) * COLS)
        wait_bytes(t.at[n, pl.ds(1, GROUPS - 1)], rz_r.at[n])
        table = t[n].reshape(SLOTS, COLS)
        mix[:, cols] = (mm(select[0], table) * weights[0] + mm(select[1], table) * weights[1]).astype(BF16)
    mixed_copy = pltpu.make_async_copy(mix, mixed_out, out_sem.at[3])
    mixed_copy.start()

    others = pl.ds(0, PLANES - 1)
    wait_bytes(zgu.at[others], send_z)
    wait_bytes(zd.at[others], send_z)
    wait_bytes(xz.at[pl.ds(0, GROUPS - 1)], send_z)
    wait_bytes(fgu.at[:, pl.ds(0, INPLANE - 1)], send_p)
    wait_bytes(fd.at[:, pl.ds(0, INPLANE - 1)], send_p)
    wait_bytes(xe.at[pl.ds(0, INPLANE - 1)], send_p)
    for n in range(NCH):
        wait_bytes(t.at[n, pl.ds(0, GROUPS - 1)], send_z)
        wait_bytes(rr.at[n, pl.ds(0, INPLANE - 1)], send_p)
    down_copy.wait()
    gate_copy.wait()
    up_copy.wait()
    mixed_copy.wait()


def body(
    tokens, norm_gain, gate_master, up_master, down_master, route_group, route_expert, route_weight
):
    vmem, hbm = pl.BlockSpec(memory_space=pltpu.VMEM), pl.BlockSpec(memory_space=pl.ANY)
    dma = pltpu.SemaphoreType.DMA
    tile = pltpu.VMEM
    return pl.pallas_call(
        kernel,
        out_shape=(
            jax.ShapeDtypeStruct((1, D, F), BF16),
            jax.ShapeDtypeStruct((1, D, F), BF16),
            jax.ShapeDtypeStruct((1, F, D), BF16),
            jax.ShapeDtypeStruct((TOK, D), BF16),
        ),
        in_specs=[hbm, hbm, hbm, vmem, hbm, vmem, vmem, vmem],
        out_specs=(hbm, hbm, hbm, hbm),
        scratch_shapes=[
            tile((3, 128, 16, 128), F32),
            tile((128, 32, 128), BF16),
            tile((128, 16, 128), BF16),
            tile((PLANES, INPLANE, 32, 128), BF16),
            tile((PLANES, INPLANE, 16, 128), BF16),
            tile((PLANES, INPLANE, 32, 128), BF16),
            tile((PLANES, INPLANE, 16, 128), BF16),
            tile((TOK, D), BF16),
            tile((GROUPS, GROUP_ROWS, D), BF16),
            tile((GROUPS, GROUP_ROWS, D), BF16),
            tile((INPLANE, PAIR_ROWS, D), BF16),
            tile((INPLANE, PAIR_ROWS, D), BF16),
            tile((EXP_ROWS, F), BF16),
            tile((F, D), BF16),
            tile((F, D), BF16),
            tile((F, D), BF16),
            tile((D, F), BF16),
            tile((D, F), BF16),
            tile((NCH, INPLANE, PAIR_ROWS, COLS), BF16),
            tile((NCH, INPLANE, PAIR_ROWS, COLS), BF16),
            tile((NCH, GROUPS, GROUP_ROWS, COLS), BF16),
            tile((NCH, GROUPS, GROUP_ROWS, COLS), BF16),
            tile((TOK, D), BF16),
            dma((4,)),
            dma((4,)),
            dma,
            dma,
            dma((PLANES,)),
            dma((PLANES,)),
            dma,
            dma((NCH,)),
            dma,
            dma,
            dma,
            dma((NCH,)),
        ],
        compiler_params=pltpu.CompilerParams(
            collective_id=0, has_side_effects=True, vmem_limit_bytes=60 * 2**20
        ),
    )(
        jnp.swapaxes(gate_master, 1, 2),
        jnp.swapaxes(up_master, 1, 2),
        down_master,
        norm_gain[None],
        tokens,
        route_group[None],
        route_expert.T,
        route_weight.T,
    )


def solution(mesh):
    placed = (
        P(("gr", "fs", "tp"), None),
        P("fs"),
        P(None, "fs", ("gr", "tp")),
        P(None, "fs", ("gr", "tp")),
        P(None, "fs", ("gr", "tp")),
        P(("gr", "fs", "tp")),
        P(("gr", "fs", "tp"), None),
        P(("gr", "fs", "tp"), None),
    )
    return jax.shard_map(
        body,
        mesh=mesh,
        in_specs=placed,
        out_specs=(
            P(("fs", "tp"), None, None),
            P(("fs", "tp"), None, None),
            P(("fs", "tp"), None, None),
            P(("gr", "fs", "tp"), None),
        ),
        check_vma=False,
    )
```

```python
import functools

import jax
import jax.numpy as jnp
from jax import lax
from jax.experimental import pallas as pl
from jax.experimental.pallas import tpu as pltpu
from jax.sharding import PartitionSpec as P

MESH = pl.DeviceIdType.MESH
BF16 = jnp.bfloat16
F32 = jnp.float32

PLANES, GROUPS, INPLANE = 8, 4, 32
TOK, D, F, CAP = 128, 2048, 256, 3
GROUP_ROWS = INPLANE * CAP
SLOTS = GROUPS * GROUP_ROWS
PAIR_ROWS = 16
EXP_ROWS = INPLANE * PAIR_ROWS
NCH = 4
PIECE = 8
PIECE_ROWS = INPLANE * PIECE
PIECES = NCH + NCH // 2
COLS = D // NCH
FAR_FIRST = (4, 3, 5, 2, 6, 1, 7)


def nt_dot(a, b):
    return lax.dot_general(a, b, (((1,), (1,)), ((), ())), preferred_element_type=F32)


def mm(a, b):
    return jnp.dot(a, b, preferred_element_type=F32)


def kernel(
    gate_in, up_in, down_in, gain, tok_in, group, expert, weight,
    gate_out, up_out, down_out, mixed_out,
    fbuf, wgu, wd, zgu, zd, fgu, fd,
    tokv, xzs, xz, xp, xe, hid,
    gt, ut, dn, go, uo, r, rr, q, t, mix,
    in_sem, out_sem, send_z, send_p, rz_gu, rz_d, rz_t, rz_r, rp_gu, rp_d, rp_t, rp_r,
):
    gr, fs, tp = lax.axis_index("gr"), lax.axis_index("fs"), lax.axis_index("tp")
    zl, x = lax.div(fs, 4), lax.rem(fs, 4)
    y, c = lax.div(tp, 2), lax.rem(tp, 2)
    z = gr * 4 + zl
    me = x * 8 + tp

    row_planes = [z] + [lax.rem(z + step, PLANES) for step in (1, 7, 2 + 4 * c)]
    row_sources = [z] + [lax.rem(z + step, PLANES) for step in (7, 1, 6 - 4 * c)]

    def z_device(target):
        return (lax.div(target, 4), lax.rem(target, 4) * 4 + x, tp)

    def hop(j):
        o = lax.rem(j * 11, INPLANE)
        tx = lax.rem(x + lax.div(o, 8), 4)
        ty = lax.rem(y + lax.rem(lax.div(o, 2), 4), 4)
        ttp = ty * 2 + lax.rem(c + lax.rem(o, 2), 2)
        return tx * 8 + ttp, (gr, zl * 4 + tx, ttp)

    def remote(src, dst, send, recv, device):
        pltpu.make_async_remote_copy(
            src_ref=src, dst_ref=dst, send_sem=send, recv_sem=recv, device_id=device, device_id_type=MESH
        ).start()

    def wait_bytes(ref, sem):
        pltpu.make_async_copy(ref, ref, sem).wait()

    barrier = pltpu.get_barrier_semaphore()
    for d in FAR_FIRST:
        pl.semaphore_signal(barrier, inc=1, device_id=z_device(lax.rem(z + d, PLANES)), device_id_type=MESH)

    @pl.loop(1, INPLANE)
    def _(j):
        pl.semaphore_signal(barrier, inc=1, device_id=hop(j)[1], device_id_type=MESH)

    inputs = [
        pltpu.make_async_copy(src, dst, in_sem.at[i])
        for i, (src, dst) in enumerate(
            ((gate_in, fbuf.at[0]), (up_in, fbuf.at[1]), (down_in, fbuf.at[2]), (tok_in, tokv))
        )
    ]
    for copy in inputs:
        copy.start()
    inputs[3].wait()

    @pl.loop(0, 4)
    def _(i):
        rows = pl.ds(i * 32, 32)
        v = tokv[rows, :].astype(F32)
        v = v * lax.rsqrt(jnp.mean(v * v, axis=-1, keepdims=True) + 1e-06)
        tokv[rows, :] = v.astype(BF16)

    ids = group[...] * INPLANE + expert[...]
    expert_iota = lax.broadcasted_iota(jnp.int32, (128, TOK), 0)
    one = [(expert_iota == ids[k : k + 1, :]).astype(F32) for k in range(2)]
    lane_iota = lax.broadcasted_iota(jnp.int32, (128, TOK), 1)
    earlier = (expert_iota < lane_iota).astype(BF16)
    count = mm((one[0] + one[1]).astype(BF16), earlier)
    slot_iota = lax.broadcasted_iota(jnp.int32, (SLOTS, TOK), 0)
    away = lax.rem(group[...] - zl + GROUPS, GROUPS)
    block = jnp.where(away == 2, 3, jnp.where(away == 3, 2, away))
    pick = []
    for k in range(2):
        rank = jnp.sum(one[k] * count, axis=0, keepdims=True).astype(jnp.int32)
        slot = jnp.where(rank < CAP, block * GROUP_ROWS + expert[k : k + 1, :] * CAP + rank, -1)
        pick.append((slot_iota == slot).astype(F32))
    rows_of = (pick[0] + pick[1]).astype(BF16)
    for n in range(NCH):
        cols = slice(n * COLS, (n + 1) * COLS)
        xzs[:, :, cols] = mm(rows_of, tokv[:, cols]).astype(BF16).reshape(GROUPS, GROUP_ROWS, COLS)
    inputs[0].wait()
    inputs[1].wait()
    scale = gain[...].reshape(1, 1, 128)

    @pl.loop(0, 16)
    def _(i):
        e = pl.ds(i * 8, 8)
        wgu[e, 0:16, :] = (fbuf[0, e] * scale).astype(BF16)
        wgu[e, 16:32, :] = (fbuf[1, e] * scale).astype(BF16)

    inputs[2].wait()

    @pl.loop(0, 16)
    def _(i):
        e = pl.ds(i * 8, 8)
        wd[e] = fbuf[2, e].astype(BF16)

    pl.semaphore_wait(barrier, len(FAR_FIRST) + INPLANE - 1)

    def send_planes(src, dst, recv, steps):
        for d in steps:
            target = lax.rem(z + d, PLANES)
            experts = pl.ds(lax.rem(target, 4) * INPLANE, INPLANE)
            remote(src.at[experts], dst.at[z], send_z, recv.at[z], z_device(target))

    def forward(src, base, dst, plane, recv):
        @pl.loop(1, INPLANE)
        def _(j):
            place, device = hop(j)
            remote(src.at[base + place], dst.at[plane, me], send_p, recv, device)

    for block in (3, 1, 2):
        remote(xzs.at[block], xz.at[block], send_z, rz_t, z_device(row_planes[block]))

    send_planes(wgu, zgu, rz_gu, FAR_FIRST)
    send_planes(wd, zd, rz_d, FAR_FIRST)
    forward(wgu, zl * INPLANE, fgu, z, rp_gu)
    forward(wd, zl * INPLANE, fd, z, rp_d)
    fgu[z, me] = wgu[zl * INPLANE + me]
    fd[z, me] = wd[zl * INPLANE + me]

    @pl.loop(0, GROUP_ROWS // 16)
    def _(i):
        rows = pl.ds(i * 16, 16)
        xz[0, rows, :] = xzs[0, rows, :]

    def relay(d, src, dst, rz, rp):
        plane = lax.rem(z + PLANES - d, PLANES)
        wait_bytes(src.at[plane], rz.at[plane])

        @pl.loop(1, INPLANE)
        def _(j):
            place, device = hop(j)
            remote(src.at[plane, place], dst.at[plane, me], send_p, rp, device)

        dst[plane, me] = src[plane, me]

    def placed(place, within):
        block = (within >= 3).astype(jnp.int32) + (within >= 6).astype(jnp.int32) + (within >= 9).astype(jnp.int32)
        at = block * GROUP_ROWS + place * CAP + within - block * CAP
        return jnp.where(within < GROUPS * CAP, at, -1)

    def onehot(mask):
        return mask.astype(F32).astype(BF16)

    wait_bytes(xz.at[pl.ds(1, GROUPS - 1)], rz_t)
    to = lax.broadcasted_iota(jnp.int32, (EXP_ROWS, SLOTS), 0)
    order = onehot(
        placed(to // PAIR_ROWS, to % PAIR_ROWS) == lax.broadcasted_iota(jnp.int32, (EXP_ROWS, SLOTS), 1)
    )
    for n in range(NCH):
        cols = slice(n * COLS, (n + 1) * COLS)
        moved = mm(order, xz[:, :, cols].reshape(SLOTS, COLS))
        xp[:, :, cols] = moved.astype(BF16).reshape(INPLANE, PAIR_ROWS, COLS)

    @pl.loop(1, INPLANE)
    def _(j):
        place, device = hop(j)
        remote(xp.at[place], xe.at[me], send_p, rp_t, device)

    xe[me] = xp[me]

    for d in FAR_FIRST:
        relay(d, zgu, fgu, rz_gu, rp_gu)

    for d in FAR_FIRST[:4]:
        relay(d, zd, fd, rz_d, rp_d)

    wait_bytes(fgu.at[:, pl.ds(0, INPLANE - 1)], rp_gu)
    for h in range(2):
        for s in range(4):
            for px in range(4):
                rows, cols = slice(h * 128, (h + 1) * 128), slice((s * 4 + px) * 128, (s * 4 + px + 1) * 128)
                tiles = slice(px * 8, (px + 1) * 8)
                gt[rows, cols] = fgu[h * 4 + s, tiles, 0:16, :].reshape(128, 128)
                ut[rows, cols] = fgu[h * 4 + s, tiles, 16:32, :].reshape(128, 128)
    wait_bytes(xe.at[pl.ds(0, INPLANE - 1)], rp_t)

    @pl.loop(0, EXP_ROWS // 128)
    def _(i):
        rows = xe[pl.ds(i * 8, 8)].reshape(128, D)
        gate = nt_dot(rows, gt[...])
        upper = nt_dot(rows, ut[...])
        hid[pl.ds(i * 128, 128), :] = (gate / (1.0 + jnp.exp(-gate)) * upper).astype(BF16)

    for d in FAR_FIRST[4:]:
        relay(d, zd, fd, rz_d, rp_d)

    wait_bytes(fd.at[:, pl.ds(0, INPLANE - 1)], rp_d)
    for h in range(2):
        for s in range(4):
            for px in range(4):
                for place in range(8):
                    col = h * 8 + place
                    dn[(s * 4 + px) * 16 : (s * 4 + px + 1) * 16, col * 128 : (col + 1) * 128] = fd[
                        h * 4 + s, px * 8 + place
                    ]
    piece_row = lax.broadcasted_iota(jnp.int32, (PIECE_ROWS, EXP_ROWS), 0)
    exp_row = lax.broadcasted_iota(jnp.int32, (PIECE_ROWS, EXP_ROWS), 1)
    tile_row = piece_row // PIECE * PAIR_ROWS
    first = mm(onehot(exp_row == tile_row + piece_row % PIECE), hid[...]).astype(BF16)
    last = mm(onehot(exp_row == tile_row + PIECE + piece_row % 4), hid[...]).astype(BF16)
    lower = lax.broadcasted_iota(jnp.int32, (PIECE_ROWS, COLS), 0) % PIECE < 4

    def send_piece(k, result):
        r[k] = result.astype(BF16).reshape(INPLANE, PIECE, COLS)

        @pl.loop(1, INPLANE)
        def _(j):
            place, device = hop(j)
            remote(r.at[k, place], rr.at[k, me], send_p, rp_r.at[k], device)

        rr[k, me] = r[k, me]

    for m in range(2):
        even, odd = (dn[:, n * COLS : (n + 1) * COLS] for n in (2 * m, 2 * m + 1))
        send_piece(2 * m, mm(first, even))
        send_piece(NCH + m, jnp.where(lower, mm(last, even), mm(last, odd)))
        send_piece(2 * m + 1, mm(first, odd))

    slot_row = lax.broadcasted_iota(jnp.int32, (SLOTS, PIECE_ROWS), 0)
    from_row = lax.broadcasted_iota(jnp.int32, (SLOTS, PIECE_ROWS), 1)
    back = onehot(placed(from_row // PIECE, from_row % PIECE) == slot_row)
    is_last = placed(from_row // PIECE, PIECE + from_row % 4) == slot_row
    back_last = [onehot(is_last & (from_row % PIECE // 4 == h)) for h in range(2)]
    for n in range(NCH):
        wait_bytes(rr.at[n, pl.ds(0, INPLANE - 1)], rp_r.at[n])
        tail = NCH + n // 2
        if n % 2 == 0:
            wait_bytes(rr.at[tail, pl.ds(0, INPLANE - 1)], rp_r.at[tail])
        moved = mm(back, rr[n].reshape(PIECE_ROWS, COLS)) + mm(back_last[n % 2], rr[tail].reshape(PIECE_ROWS, COLS))
        q[n] = moved.astype(BF16).reshape(GROUPS, GROUP_ROWS, COLS)
        for block in (3, 1, 2):
            remote(q.at[n, block], t.at[n, block], send_z, rz_r.at[n], z_device(row_sources[block]))

        t[n, 0] = q[n, 0]

    down_copy = pltpu.make_async_copy(dn, down_out.at[0], out_sem.at[2])
    down_copy.start()
    for h in range(2):
        for s in range(16):
            rows, cols = slice(h * 128, (h + 1) * 128), slice(s * 128, (s + 1) * 128)
            go[cols, rows] = gt[rows, cols].T
            uo[cols, rows] = ut[rows, cols].T
    gate_copy = pltpu.make_async_copy(go, gate_out.at[0], out_sem.at[0])
    up_copy = pltpu.make_async_copy(uo, up_out.at[0], out_sem.at[1])
    gate_copy.start()
    up_copy.start()

    select = [p.T.astype(BF16) for p in pick]
    weights = [jnp.broadcast_to(weight[k : k + 1, :], (128, TOK)).T[:, 0:1] for k in range(2)]
    for n in range(NCH):
        cols = slice(n * COLS, (n + 1) * COLS)
        wait_bytes(t.at[n, pl.ds(1, GROUPS - 1)], rz_r.at[n])
        table = t[n].reshape(SLOTS, COLS)
        mix[:, cols] = (mm(select[0], table) * weights[0] + mm(select[1], table) * weights[1]).astype(BF16)
    mixed_copy = pltpu.make_async_copy(mix, mixed_out, out_sem.at[3])
    mixed_copy.start()

    others = pl.ds(0, PLANES - 1)
    wait_bytes(zgu.at[others], send_z)
    wait_bytes(zd.at[others], send_z)
    wait_bytes(xz.at[pl.ds(0, GROUPS - 1)], send_z)
    wait_bytes(fgu.at[:, pl.ds(0, INPLANE - 1)], send_p)
    wait_bytes(fd.at[:, pl.ds(0, INPLANE - 1)], send_p)
    wait_bytes(xe.at[pl.ds(0, INPLANE - 1)], send_p)
    for n in range(NCH):
        wait_bytes(t.at[n, pl.ds(0, GROUPS - 1)], send_z)
    for k in range(PIECES):
        wait_bytes(rr.at[k, pl.ds(0, INPLANE - 1)], send_p)
    down_copy.wait()
    gate_copy.wait()
    up_copy.wait()
    mixed_copy.wait()


def write_out(*refs):
    srcs, dsts, bufs, in_sem, out_sem = refs[0:4], refs[4:8], refs[8:12], refs[12], refs[13]
    pieces = []
    for i in range(4):
        rows = srcs[i].shape[-2] // 2
        for h in range(2):
            cut = (0,) * (len(srcs[i].shape) - 2) + (pl.ds(h * rows, rows),)
            n = 2 * i + h
            pieces.append((
                pltpu.make_async_copy(srcs[i].at[cut], bufs[i].at[cut], in_sem.at[n]),
                pltpu.make_async_copy(bufs[i].at[cut], dsts[i].at[cut], out_sem.at[n]),
            ))
    for load, _ in pieces:
        load.start()
    for load, store in pieces:
        load.wait()
        store.start()
    for _, store in pieces:
        store.wait()


def body(
    tokens, norm_gain, gate_master, up_master, down_master, route_group, route_expert, route_weight
):
    vmem, hbm = pl.BlockSpec(memory_space=pltpu.VMEM), pl.BlockSpec(memory_space=pltpu.HBM)
    dma = pltpu.SemaphoreType.DMA
    tile = pltpu.VMEM
    shapes = (
        jax.ShapeDtypeStruct((1, D, F), BF16),
        jax.ShapeDtypeStruct((1, D, F), BF16),
        jax.ShapeDtypeStruct((1, F, D), BF16),
        jax.ShapeDtypeStruct((TOK, D), BF16),
    )
    outs = pl.pallas_call(
        kernel,
        out_shape=shapes,
        in_specs=[hbm, hbm, hbm, vmem, hbm, vmem, vmem, vmem],
        out_specs=(hbm,) * 4,
        scratch_shapes=[
            tile((3, 128, 16, 128), F32),
            tile((128, 32, 128), BF16),
            tile((128, 16, 128), BF16),
            tile((PLANES, INPLANE, 32, 128), BF16),
            tile((PLANES, INPLANE, 16, 128), BF16),
            tile((PLANES, INPLANE, 32, 128), BF16),
            tile((PLANES, INPLANE, 16, 128), BF16),
            tile((TOK, D), BF16),
            tile((GROUPS, GROUP_ROWS, D), BF16),
            tile((GROUPS, GROUP_ROWS, D), BF16),
            tile((INPLANE, PAIR_ROWS, D), BF16),
            tile((INPLANE, PAIR_ROWS, D), BF16),
            tile((EXP_ROWS, F), BF16),
            tile((F, D), BF16),
            tile((F, D), BF16),
            tile((F, D), BF16),
            tile((D, F), BF16),
            tile((D, F), BF16),
            tile((PIECES, INPLANE, PIECE, COLS), BF16),
            tile((PIECES, INPLANE, PIECE, COLS), BF16),
            tile((NCH, GROUPS, GROUP_ROWS, COLS), BF16),
            tile((NCH, GROUPS, GROUP_ROWS, COLS), BF16),
            tile((TOK, D), BF16),
            dma((4,)),
            dma((4,)),
            dma,
            dma,
            dma((PLANES,)),
            dma((PLANES,)),
            dma,
            dma((NCH,)),
            dma,
            dma,
            dma,
            dma((PIECES,)),
        ],
        compiler_params=pltpu.CompilerParams(
            collective_id=0, has_side_effects=True, vmem_limit_bytes=60 * 2**20
        ),
    )(
        jnp.swapaxes(gate_master, 1, 2),
        jnp.swapaxes(up_master, 1, 2),
        down_master,
        norm_gain[None],
        tokens,
        route_group[None],
        route_expert.T,
        route_weight.T,
    )
    return pl.pallas_call(
        write_out,
        out_shape=shapes,
        in_specs=[hbm] * 4,
        out_specs=(hbm,) * 4,
        scratch_shapes=[tile(a.shape, a.dtype) for a in shapes] + [dma((8,)), dma((8,))],
        compiler_params=pltpu.CompilerParams(vmem_limit_bytes=60 * 2**20),
    )(*outs)


def solution(mesh):
    placed = (
        P(("gr", "fs", "tp"), None),
        P("fs"),
        P(None, "fs", ("gr", "tp")),
        P(None, "fs", ("gr", "tp")),
        P(None, "fs", ("gr", "tp")),
        P(("gr", "fs", "tp")),
        P(("gr", "fs", "tp"), None),
        P(("gr", "fs", "tp"), None),
    )
    return jax.shard_map(
        body,
        mesh=mesh,
        in_specs=placed,
        out_specs=(
            P(("fs", "tp"), None, None),
            P(("fs", "tp"), None, None),
            P(("fs", "tp"), None, None),
            P(("gr", "fs", "tp"), None),
        ),
        check_vma=False,
    )
```

```python
import functools

import jax
import jax.numpy as jnp
from jax import lax
from jax.experimental import pallas as pl
from jax.experimental.pallas import tpu as pltpu
from jax.sharding import PartitionSpec as P

MESH = pl.DeviceIdType.MESH
BF16 = jnp.bfloat16
F32 = jnp.float32

PLANES, GROUPS, INPLANE = 8, 4, 32
TOK, D, F, CAP = 128, 2048, 256, 3
GROUP_ROWS = INPLANE * CAP
SLOTS = GROUPS * GROUP_ROWS
PAIR_ROWS = 16
EXP_ROWS = INPLANE * PAIR_ROWS
NCH = 4
PIECE = 8
PIECE_ROWS = INPLANE * PIECE
PIECES = NCH + NCH // 2
COLS = D // NCH
NEAR_FIRST = (1, 7, 2, 6, 3, 5, 4)


def nt_dot(a, b):
    return lax.dot_general(a, b, (((1,), (1,)), ((), ())), preferred_element_type=F32)


def mm(a, b):
    return jnp.dot(a, b, preferred_element_type=F32)


def kernel(
    gate_in, up_in, down_in, gain, tok_in, group, expert, weight,
    gate_out, up_out, down_out, mixed_out,
    fbuf, wgu, wd, zgu, zd, fgu, fd,
    tokv, xzs, xz, xp, xe, hid,
    gt, ut, dn, go, uo, r, rr, q, t, mix,
    in_sem, out_sem, send_z, send_p, rz_gu, rz_d, rz_t, rz_r, rp_gu, rp_d, rp_t, rp_r,
):
    gr, fs, tp = lax.axis_index("gr"), lax.axis_index("fs"), lax.axis_index("tp")
    zl, x = lax.div(fs, 4), lax.rem(fs, 4)
    y, c = lax.div(tp, 2), lax.rem(tp, 2)
    z = gr * 4 + zl
    me = x * 8 + tp

    row_planes = [z] + [lax.rem(z + step, PLANES) for step in (1, 7, 2 + 4 * c)]
    row_sources = [z] + [lax.rem(z + step, PLANES) for step in (7, 1, 6 - 4 * c)]

    def z_device(target):
        return (lax.div(target, 4), lax.rem(target, 4) * 4 + x, tp)

    def hop(j):
        o = lax.rem(j * 21, INPLANE)
        tx = lax.rem(x + lax.div(o, 8), 4)
        ty = lax.rem(y + lax.rem(lax.div(o, 2), 4), 4)
        ttp = ty * 2 + lax.rem(c + lax.rem(o, 2), 2)
        return tx * 8 + ttp, (gr, zl * 4 + tx, ttp)

    def remote(src, dst, send, recv, device):
        pltpu.make_async_remote_copy(
            src_ref=src, dst_ref=dst, send_sem=send, recv_sem=recv, device_id=device, device_id_type=MESH
        ).start()

    def wait_bytes(ref, sem):
        pltpu.make_async_copy(ref, ref, sem).wait()

    barrier = pltpu.get_barrier_semaphore()
    for d in NEAR_FIRST:
        pl.semaphore_signal(barrier, inc=1, device_id=z_device(lax.rem(z + d, PLANES)), device_id_type=MESH)

    @pl.loop(1, INPLANE)
    def _(j):
        pl.semaphore_signal(barrier, inc=1, device_id=hop(j)[1], device_id_type=MESH)

    inputs = [
        pltpu.make_async_copy(src, dst, in_sem.at[i])
        for i, (src, dst) in enumerate(
            ((gate_in, fbuf.at[0]), (up_in, fbuf.at[1]), (down_in, fbuf.at[2]), (tok_in, tokv))
        )
    ]
    for copy in inputs:
        copy.start()
    inputs[3].wait()

    @pl.loop(0, 4)
    def _(i):
        rows = pl.ds(i * 32, 32)
        v = tokv[rows, :].astype(F32)
        v = v * lax.rsqrt(jnp.mean(v * v, axis=-1, keepdims=True) + 1e-06)
        tokv[rows, :] = v.astype(BF16)

    ids = group[...] * INPLANE + expert[...]
    expert_iota = lax.broadcasted_iota(jnp.int32, (128, TOK), 0)
    one = [(expert_iota == ids[k : k + 1, :]).astype(F32) for k in range(2)]
    lane_iota = lax.broadcasted_iota(jnp.int32, (128, TOK), 1)
    earlier = (expert_iota < lane_iota).astype(BF16)
    count = mm((one[0] + one[1]).astype(BF16), earlier)
    slot_iota = lax.broadcasted_iota(jnp.int32, (SLOTS, TOK), 0)
    away = lax.rem(group[...] - zl + GROUPS, GROUPS)
    block = jnp.where(away == 2, 3, jnp.where(away == 3, 2, away))
    pick = []
    for k in range(2):
        rank = jnp.sum(one[k] * count, axis=0, keepdims=True).astype(jnp.int32)
        slot = jnp.where(rank < CAP, block * GROUP_ROWS + expert[k : k + 1, :] * CAP + rank, -1)
        pick.append((slot_iota == slot).astype(F32))
    rows_of = (pick[0] + pick[1]).astype(BF16)
    for n in range(NCH):
        cols = slice(n * COLS, (n + 1) * COLS)
        xzs[:, :, cols] = mm(rows_of, tokv[:, cols]).astype(BF16).reshape(GROUPS, GROUP_ROWS, COLS)
    inputs[0].wait()
    inputs[1].wait()
    scale = gain[...].reshape(1, 1, 128)

    @pl.loop(0, 16)
    def _(i):
        e = pl.ds(i * 8, 8)
        wgu[e, 0:16, :] = (fbuf[0, e] * scale).astype(BF16)
        wgu[e, 16:32, :] = (fbuf[1, e] * scale).astype(BF16)

    inputs[2].wait()

    @pl.loop(0, 16)
    def _(i):
        e = pl.ds(i * 8, 8)
        wd[e] = fbuf[2, e].astype(BF16)

    pl.semaphore_wait(barrier, len(NEAR_FIRST) + INPLANE - 1)

    def send_planes(src, dst, recv, steps):
        for d in steps:
            target = lax.rem(z + d, PLANES)
            experts = pl.ds(lax.rem(target, 4) * INPLANE, INPLANE)
            remote(src.at[experts], dst.at[z], send_z, recv.at[z], z_device(target))

    def forward(src, base, dst, plane, recv):
        @pl.loop(1, INPLANE)
        def _(j):
            place, device = hop(j)
            remote(src.at[base + place], dst.at[plane, me], send_p, recv, device)

    for block in (3, 1, 2):
        remote(xzs.at[block], xz.at[block], send_z, rz_t, z_device(row_planes[block]))

    send_planes(wgu, zgu, rz_gu, NEAR_FIRST)
    send_planes(wd, zd, rz_d, NEAR_FIRST)
    forward(wgu, zl * INPLANE, fgu, z, rp_gu)
    forward(wd, zl * INPLANE, fd, z, rp_d)
    fgu[z, me] = wgu[zl * INPLANE + me]
    fd[z, me] = wd[zl * INPLANE + me]

    @pl.loop(0, GROUP_ROWS // 16)
    def _(i):
        rows = pl.ds(i * 16, 16)
        xz[0, rows, :] = xzs[0, rows, :]

    def relay(d, src, dst, rz, rp):
        plane = lax.rem(z + PLANES - d, PLANES)
        wait_bytes(src.at[plane], rz.at[plane])

        @pl.loop(1, INPLANE)
        def _(j):
            place, device = hop(j)
            remote(src.at[plane, place], dst.at[plane, me], send_p, rp, device)

        dst[plane, me] = src[plane, me]

    def placed(place, within):
        block = (within >= 3).astype(jnp.int32) + (within >= 6).astype(jnp.int32) + (within >= 9).astype(jnp.int32)
        at = block * GROUP_ROWS + place * CAP + within - block * CAP
        return jnp.where(within < GROUPS * CAP, at, -1)

    def onehot(mask):
        return mask.astype(F32).astype(BF16)

    wait_bytes(xz.at[pl.ds(1, GROUPS - 1)], rz_t)
    to = lax.broadcasted_iota(jnp.int32, (EXP_ROWS, SLOTS), 0)
    order = onehot(
        placed(to // PAIR_ROWS, to % PAIR_ROWS) == lax.broadcasted_iota(jnp.int32, (EXP_ROWS, SLOTS), 1)
    )
    for n in range(NCH):
        cols = slice(n * COLS, (n + 1) * COLS)
        moved = mm(order, xz[:, :, cols].reshape(SLOTS, COLS))
        xp[:, :, cols] = moved.astype(BF16).reshape(INPLANE, PAIR_ROWS, COLS)

    @pl.loop(1, INPLANE)
    def _(j):
        place, device = hop(j)
        remote(xp.at[place], xe.at[me], send_p, rp_t, device)

    xe[me] = xp[me]

    for d in NEAR_FIRST:
        relay(d, zgu, fgu, rz_gu, rp_gu)

    for d in NEAR_FIRST[:4]:
        relay(d, zd, fd, rz_d, rp_d)

    wait_bytes(fgu.at[:, pl.ds(0, INPLANE - 1)], rp_gu)
    for h in range(2):
        for s in range(4):
            for px in range(4):
                rows, cols = slice(h * 128, (h + 1) * 128), slice((s * 4 + px) * 128, (s * 4 + px + 1) * 128)
                tiles = slice(px * 8, (px + 1) * 8)
                gt[rows, cols] = fgu[h * 4 + s, tiles, 0:16, :].reshape(128, 128)
                ut[rows, cols] = fgu[h * 4 + s, tiles, 16:32, :].reshape(128, 128)
    wait_bytes(xe.at[pl.ds(0, INPLANE - 1)], rp_t)

    @pl.loop(0, EXP_ROWS // 128)
    def _(i):
        rows = xe[pl.ds(i * 8, 8)].reshape(128, D)
        gate = nt_dot(rows, gt[...])
        upper = nt_dot(rows, ut[...])
        hid[pl.ds(i * 128, 128), :] = (gate / (1.0 + jnp.exp(-gate)) * upper).astype(BF16)

    for d in NEAR_FIRST[4:]:
        relay(d, zd, fd, rz_d, rp_d)

    wait_bytes(fd.at[:, pl.ds(0, INPLANE - 1)], rp_d)
    for h in range(2):
        for s in range(4):
            for px in range(4):
                for place in range(8):
                    col = h * 8 + place
                    dn[(s * 4 + px) * 16 : (s * 4 + px + 1) * 16, col * 128 : (col + 1) * 128] = fd[
                        h * 4 + s, px * 8 + place
                    ]
    piece_row = lax.broadcasted_iota(jnp.int32, (PIECE_ROWS, EXP_ROWS), 0)
    exp_row = lax.broadcasted_iota(jnp.int32, (PIECE_ROWS, EXP_ROWS), 1)
    tile_row = piece_row // PIECE * PAIR_ROWS
    first = mm(onehot(exp_row == tile_row + piece_row % PIECE), hid[...]).astype(BF16)
    last = mm(onehot(exp_row == tile_row + PIECE + piece_row % 4), hid[...]).astype(BF16)
    lower = lax.broadcasted_iota(jnp.int32, (PIECE_ROWS, COLS), 0) % PIECE < 4

    def send_piece(k, result):
        r[k] = result.astype(BF16).reshape(INPLANE, PIECE, COLS)

        @pl.loop(1, INPLANE)
        def _(j):
            place, device = hop(j)
            remote(r.at[k, place], rr.at[k, me], send_p, rp_r.at[k], device)

        rr[k, me] = r[k, me]

    for m in range(2):
        even, odd = (dn[:, n * COLS : (n + 1) * COLS] for n in (2 * m, 2 * m + 1))
        send_piece(2 * m, mm(first, even))
        send_piece(NCH + m, jnp.where(lower, mm(last, even), mm(last, odd)))
        send_piece(2 * m + 1, mm(first, odd))

    slot_row = lax.broadcasted_iota(jnp.int32, (SLOTS, PIECE_ROWS), 0)
    from_row = lax.broadcasted_iota(jnp.int32, (SLOTS, PIECE_ROWS), 1)
    back = onehot(placed(from_row // PIECE, from_row % PIECE) == slot_row)
    is_last = placed(from_row // PIECE, PIECE + from_row % 4) == slot_row
    back_last = [onehot(is_last & (from_row % PIECE // 4 == h)) for h in range(2)]
    for n in range(NCH):
        wait_bytes(rr.at[n, pl.ds(0, INPLANE - 1)], rp_r.at[n])
        tail = NCH + n // 2
        if n % 2 == 0:
            wait_bytes(rr.at[tail, pl.ds(0, INPLANE - 1)], rp_r.at[tail])
        moved = mm(back, rr[n].reshape(PIECE_ROWS, COLS)) + mm(back_last[n % 2], rr[tail].reshape(PIECE_ROWS, COLS))
        q[n] = moved.astype(BF16).reshape(GROUPS, GROUP_ROWS, COLS)
        for block in (3, 1, 2):
            remote(q.at[n, block], t.at[n, block], send_z, rz_r.at[n], z_device(row_sources[block]))

        t[n, 0] = q[n, 0]

    down_copy = pltpu.make_async_copy(dn, down_out.at[0], out_sem.at[2])
    down_copy.start()
    for h in range(2):
        for s in range(16):
            rows, cols = slice(h * 128, (h + 1) * 128), slice(s * 128, (s + 1) * 128)
            go[cols, rows] = gt[rows, cols].T
            uo[cols, rows] = ut[rows, cols].T
    gate_copy = pltpu.make_async_copy(go, gate_out.at[0], out_sem.at[0])
    up_copy = pltpu.make_async_copy(uo, up_out.at[0], out_sem.at[1])
    gate_copy.start()
    up_copy.start()

    select = [p.T.astype(BF16) for p in pick]
    weights = [jnp.broadcast_to(weight[k : k + 1, :], (128, TOK)).T[:, 0:1] for k in range(2)]
    for n in range(NCH):
        cols = slice(n * COLS, (n + 1) * COLS)
        wait_bytes(t.at[n, pl.ds(1, GROUPS - 1)], rz_r.at[n])
        table = t[n].reshape(SLOTS, COLS)
        mix[:, cols] = (mm(select[0], table) * weights[0] + mm(select[1], table) * weights[1]).astype(BF16)
    mixed_copy = pltpu.make_async_copy(mix, mixed_out, out_sem.at[3])
    mixed_copy.start()

    others = pl.ds(0, PLANES - 1)
    wait_bytes(zgu.at[others], send_z)
    wait_bytes(zd.at[others], send_z)
    wait_bytes(xz.at[pl.ds(0, GROUPS - 1)], send_z)
    wait_bytes(fgu.at[:, pl.ds(0, INPLANE - 1)], send_p)
    wait_bytes(fd.at[:, pl.ds(0, INPLANE - 1)], send_p)
    wait_bytes(xe.at[pl.ds(0, INPLANE - 1)], send_p)
    for n in range(NCH):
        wait_bytes(t.at[n, pl.ds(0, GROUPS - 1)], send_z)
    for k in range(PIECES):
        wait_bytes(rr.at[k, pl.ds(0, INPLANE - 1)], send_p)
    down_copy.wait()
    gate_copy.wait()
    up_copy.wait()
    mixed_copy.wait()


def write_out(*refs):
    srcs, dsts, bufs, in_sem, out_sem = refs[0:4], refs[4:8], refs[8:12], refs[12], refs[13]
    pieces = []
    for i in range(4):
        rows = srcs[i].shape[-2] // 2
        for h in range(2):
            cut = (0,) * (len(srcs[i].shape) - 2) + (pl.ds(h * rows, rows),)
            n = 2 * i + h
            pieces.append((
                pltpu.make_async_copy(srcs[i].at[cut], bufs[i].at[cut], in_sem.at[n]),
                pltpu.make_async_copy(bufs[i].at[cut], dsts[i].at[cut], out_sem.at[n]),
            ))
    for load, _ in pieces:
        load.start()
    for load, store in pieces:
        load.wait()
        store.start()
    for _, store in pieces:
        store.wait()


def body(
    tokens, norm_gain, gate_master, up_master, down_master, route_group, route_expert, route_weight
):
    vmem, hbm = pl.BlockSpec(memory_space=pltpu.VMEM), pl.BlockSpec(memory_space=pltpu.HBM)
    dma = pltpu.SemaphoreType.DMA
    tile = pltpu.VMEM
    shapes = (
        jax.ShapeDtypeStruct((1, D, F), BF16),
        jax.ShapeDtypeStruct((1, D, F), BF16),
        jax.ShapeDtypeStruct((1, F, D), BF16),
        jax.ShapeDtypeStruct((TOK, D), BF16),
    )
    outs = pl.pallas_call(
        kernel,
        out_shape=shapes,
        in_specs=[hbm, hbm, hbm, vmem, hbm, vmem, vmem, vmem],
        out_specs=(hbm,) * 4,
        scratch_shapes=[
            tile((3, 128, 16, 128), F32),
            tile((128, 32, 128), BF16),
            tile((128, 16, 128), BF16),
            tile((PLANES, INPLANE, 32, 128), BF16),
            tile((PLANES, INPLANE, 16, 128), BF16),
            tile((PLANES, INPLANE, 32, 128), BF16),
            tile((PLANES, INPLANE, 16, 128), BF16),
            tile((TOK, D), BF16),
            tile((GROUPS, GROUP_ROWS, D), BF16),
            tile((GROUPS, GROUP_ROWS, D), BF16),
            tile((INPLANE, PAIR_ROWS, D), BF16),
            tile((INPLANE, PAIR_ROWS, D), BF16),
            tile((EXP_ROWS, F), BF16),
            tile((F, D), BF16),
            tile((F, D), BF16),
            tile((F, D), BF16),
            tile((D, F), BF16),
            tile((D, F), BF16),
            tile((PIECES, INPLANE, PIECE, COLS), BF16),
            tile((PIECES, INPLANE, PIECE, COLS), BF16),
            tile((NCH, GROUPS, GROUP_ROWS, COLS), BF16),
            tile((NCH, GROUPS, GROUP_ROWS, COLS), BF16),
            tile((TOK, D), BF16),
            dma((4,)),
            dma((4,)),
            dma,
            dma,
            dma((PLANES,)),
            dma((PLANES,)),
            dma,
            dma((NCH,)),
            dma,
            dma,
            dma,
            dma((PIECES,)),
        ],
        compiler_params=pltpu.CompilerParams(
            collective_id=0, has_side_effects=True, vmem_limit_bytes=60 * 2**20
        ),
    )(
        jnp.swapaxes(gate_master, 1, 2),
        jnp.swapaxes(up_master, 1, 2),
        down_master,
        norm_gain[None],
        tokens,
        route_group[None],
        route_expert.T,
        route_weight.T,
    )
    return pl.pallas_call(
        write_out,
        out_shape=shapes,
        in_specs=[hbm] * 4,
        out_specs=(hbm,) * 4,
        scratch_shapes=[tile(a.shape, a.dtype) for a in shapes] + [dma((8,)), dma((8,))],
        compiler_params=pltpu.CompilerParams(vmem_limit_bytes=60 * 2**20),
    )(*outs)


def solution(mesh):
    placed = (
        P(("gr", "fs", "tp"), None),
        P("fs"),
        P(None, "fs", ("gr", "tp")),
        P(None, "fs", ("gr", "tp")),
        P(None, "fs", ("gr", "tp")),
        P(("gr", "fs", "tp")),
        P(("gr", "fs", "tp"), None),
        P(("gr", "fs", "tp"), None),
    )
    return jax.shard_map(
        body,
        mesh=mesh,
        in_specs=placed,
        out_specs=(
            P(("fs", "tp"), None, None),
            P(("fs", "tp"), None, None),
            P(("fs", "tp"), None, None),
            P(("gr", "fs", "tp"), None),
        ),
        check_vma=False,
    )
```

```python
import functools

import jax
import jax.numpy as jnp
from jax import lax
from jax.experimental import pallas as pl
from jax.experimental.pallas import tpu as pltpu
from jax.sharding import PartitionSpec as P

MESH = pl.DeviceIdType.MESH
BF16 = jnp.bfloat16
F32 = jnp.float32

PLANES, GROUPS, INPLANE = 8, 4, 32
TOK, D, F, CAP = 128, 2048, 256, 3
GROUP_ROWS = INPLANE * CAP
SLOTS = GROUPS * GROUP_ROWS
NCH = 4
PIECE = 8
PIECE_ROWS = INPLANE * PIECE
PIECES = NCH + NCH // 2
COLS = D // NCH
NEAR_FIRST = (1, 7, 2, 6, 3, 5, 4)


def nt_dot(a, b):
    return lax.dot_general(a, b, (((1,), (1,)), ((), ())), preferred_element_type=F32)


def mm(a, b):
    return jnp.dot(a, b, preferred_element_type=F32)


def kernel(
    gate_in, up_in, down_in, gain, tok_in, group, expert, weight,
    gate_out, up_out, down_out, mixed_out,
    fbuf, wgu, wd, zgu, zd, fgu, fd,
    tokv, xzs, xz, xp, xpl, xe, xel, xl, hid, hidl,
    gt, ut, dn, go, uo, r, rr, q, t, mix,
    in_sem, out_sem, send_z, send_p, rz_gu, rz_d, rz_t, rz_r, rp_gu, rp_d, rp_t, rp_r,
):
    gr, fs, tp = lax.axis_index("gr"), lax.axis_index("fs"), lax.axis_index("tp")
    zl, x = lax.div(fs, 4), lax.rem(fs, 4)
    y, c = lax.div(tp, 2), lax.rem(tp, 2)
    z = gr * 4 + zl
    me = x * 8 + tp

    row_planes = [z] + [lax.rem(z + step, PLANES) for step in (1, 7, 2 + 4 * c)]
    row_sources = [z] + [lax.rem(z + step, PLANES) for step in (7, 1, 6 - 4 * c)]

    def z_device(target):
        return (lax.div(target, 4), lax.rem(target, 4) * 4 + x, tp)

    def hop(j):
        o = lax.rem(j * 21, INPLANE)
        tx = lax.rem(x + lax.div(o, 8), 4)
        ty = lax.rem(y + lax.rem(lax.div(o, 2), 4), 4)
        ttp = ty * 2 + lax.rem(c + lax.rem(o, 2), 2)
        return tx * 8 + ttp, (gr, zl * 4 + tx, ttp)

    def remote(src, dst, send, recv, device):
        pltpu.make_async_remote_copy(
            src_ref=src, dst_ref=dst, send_sem=send, recv_sem=recv, device_id=device, device_id_type=MESH
        ).start()

    def wait_bytes(ref, sem):
        pltpu.make_async_copy(ref, ref, sem).wait()

    barrier = pltpu.get_barrier_semaphore()
    for d in NEAR_FIRST:
        pl.semaphore_signal(barrier, inc=1, device_id=z_device(lax.rem(z + d, PLANES)), device_id_type=MESH)

    @pl.loop(1, INPLANE)
    def _(j):
        pl.semaphore_signal(barrier, inc=1, device_id=hop(j)[1], device_id_type=MESH)

    inputs = [
        pltpu.make_async_copy(src, dst, in_sem.at[i])
        for i, (src, dst) in enumerate(
            ((gate_in, fbuf.at[0]), (up_in, fbuf.at[1]), (down_in, fbuf.at[2]), (tok_in, tokv))
        )
    ]
    for copy in inputs:
        copy.start()
    inputs[3].wait()

    @pl.loop(0, 4)
    def _(i):
        rows = pl.ds(i * 32, 32)
        v = tokv[rows, :].astype(F32)
        v = v * lax.rsqrt(jnp.mean(v * v, axis=-1, keepdims=True) + 1e-06)
        tokv[rows, :] = v.astype(BF16)

    ids = group[...] * INPLANE + expert[...]
    expert_iota = lax.broadcasted_iota(jnp.int32, (128, TOK), 0)
    one = [(expert_iota == ids[k : k + 1, :]).astype(F32) for k in range(2)]
    lane_iota = lax.broadcasted_iota(jnp.int32, (128, TOK), 1)
    earlier = (expert_iota < lane_iota).astype(BF16)
    count = mm((one[0] + one[1]).astype(BF16), earlier)
    slot_iota = lax.broadcasted_iota(jnp.int32, (SLOTS, TOK), 0)
    away = lax.rem(group[...] - zl + GROUPS, GROUPS)
    block = jnp.where(away == 2, 3, jnp.where(away == 3, 2, away))
    pick = []
    for k in range(2):
        rank = jnp.sum(one[k] * count, axis=0, keepdims=True).astype(jnp.int32)
        slot = jnp.where(rank < CAP, block * GROUP_ROWS + expert[k : k + 1, :] * CAP + rank, -1)
        pick.append((slot_iota == slot).astype(F32))
    rows_of = (pick[0] + pick[1]).astype(BF16)
    for n in range(NCH):
        cols = slice(n * COLS, (n + 1) * COLS)
        xzs[:, :, cols] = mm(rows_of, tokv[:, cols]).astype(BF16).reshape(GROUPS, GROUP_ROWS, COLS)
    inputs[0].wait()
    inputs[1].wait()
    scale = gain[...].reshape(1, 1, 128)

    @pl.loop(0, 16)
    def _(i):
        e = pl.ds(i * 8, 8)
        wgu[e, 0:16, :] = (fbuf[0, e] * scale).astype(BF16)
        wgu[e, 16:32, :] = (fbuf[1, e] * scale).astype(BF16)

    inputs[2].wait()

    @pl.loop(0, 16)
    def _(i):
        e = pl.ds(i * 8, 8)
        wd[e] = fbuf[2, e].astype(BF16)

    pl.semaphore_wait(barrier, len(NEAR_FIRST) + INPLANE - 1)

    def send_planes(src, dst, recv, steps):
        for d in steps:
            target = lax.rem(z + d, PLANES)
            experts = pl.ds(lax.rem(target, 4) * INPLANE, INPLANE)
            remote(src.at[experts], dst.at[z], send_z, recv.at[z], z_device(target))

    def forward(src, base, dst, plane, recv):
        @pl.loop(1, INPLANE)
        def _(j):
            place, device = hop(j)
            remote(src.at[base + place], dst.at[plane, me], send_p, recv, device)

    for block in (3, 1, 2):
        remote(xzs.at[block], xz.at[block], send_z, rz_t, z_device(row_planes[block]))

    send_planes(wgu, zgu, rz_gu, NEAR_FIRST)
    send_planes(wd, zd, rz_d, NEAR_FIRST)
    forward(wgu, zl * INPLANE, fgu, z, rp_gu)
    forward(wd, zl * INPLANE, fd, z, rp_d)
    fgu[z, me] = wgu[zl * INPLANE + me]
    fd[z, me] = wd[zl * INPLANE + me]

    @pl.loop(0, GROUP_ROWS // 16)
    def _(i):
        rows = pl.ds(i * 16, 16)
        xz[0, rows, :] = xzs[0, rows, :]

    def relay(d, src, dst, rz, rp):
        plane = lax.rem(z + PLANES - d, PLANES)
        wait_bytes(src.at[plane], rz.at[plane])

        @pl.loop(1, INPLANE)
        def _(j):
            place, device = hop(j)
            remote(src.at[plane, place], dst.at[plane, me], send_p, rp, device)

        dst[plane, me] = src[plane, me]

    def placed(place, within):
        block = (within >= 3).astype(jnp.int32) + (within >= 6).astype(jnp.int32) + (within >= 9).astype(jnp.int32)
        at = block * GROUP_ROWS + place * CAP + within - block * CAP
        return jnp.where(within < GROUPS * CAP, at, -1)

    def onehot(mask):
        return mask.astype(F32).astype(BF16)

    wait_bytes(xz.at[pl.ds(1, GROUPS - 1)], rz_t)
    to = lax.broadcasted_iota(jnp.int32, (PIECE_ROWS, SLOTS), 0)
    of = lax.broadcasted_iota(jnp.int32, (PIECE_ROWS, SLOTS), 1)
    order = onehot(placed(to // PIECE, to % PIECE) == of)
    order_last = onehot(placed(to // PIECE, PIECE + to % 4) == of)
    lower = lax.broadcasted_iota(jnp.int32, (PIECE_ROWS, COLS), 0) % PIECE < 4
    halves = []
    for n in range(NCH):
        cols = slice(n * COLS, (n + 1) * COLS)
        rows = xz[:, :, cols].reshape(SLOTS, COLS)
        xp[:, :, cols] = mm(order, rows).astype(BF16).reshape(INPLANE, PIECE, COLS)
        halves.append(mm(order_last, rows))
    for m in range(NCH // 2):
        both = jnp.where(lower, halves[m], halves[m + NCH // 2])
        xpl[:, :, m * COLS : (m + 1) * COLS] = both.astype(BF16).reshape(INPLANE, PIECE, COLS)

    @pl.loop(1, INPLANE)
    def _(j):
        place, device = hop(j)
        remote(xp.at[place], xe.at[me], send_p, rp_t.at[0], device)
        remote(xpl.at[place], xel.at[me], send_p, rp_t.at[1], device)

    xe[me] = xp[me]
    xel[me] = xpl[me]

    for d in NEAR_FIRST:
        relay(d, zgu, fgu, rz_gu, rp_gu)

    for d in NEAR_FIRST[:4]:
        relay(d, zd, fd, rz_d, rp_d)

    wait_bytes(fgu.at[:, pl.ds(0, INPLANE - 1)], rp_gu)
    for h in range(2):
        for s in range(4):
            for px in range(4):
                rows, cols = slice(h * 128, (h + 1) * 128), slice((s * 4 + px) * 128, (s * 4 + px + 1) * 128)
                tiles = slice(px * 8, (px + 1) * 8)
                gt[rows, cols] = fgu[h * 4 + s, tiles, 0:16, :].reshape(128, 128)
                ut[rows, cols] = fgu[h * 4 + s, tiles, 16:32, :].reshape(128, 128)
    wait_bytes(xe.at[pl.ds(0, INPLANE - 1)], rp_t.at[0])
    wait_bytes(xel.at[pl.ds(0, INPLANE - 1)], rp_t.at[1])

    def hidden(rows):
        gate = nt_dot(rows, gt[...])
        upper = nt_dot(rows, ut[...])
        return (gate / (1.0 + jnp.exp(-gate)) * upper).astype(BF16)

    @pl.loop(0, PIECE_ROWS // 128)
    def _(i):
        hid[pl.ds(i * 128, 128), :] = hidden(xe[pl.ds(i * 16, 16)].reshape(128, D))

    last_row = lax.broadcasted_iota(jnp.int32, (128, PIECE_ROWS), 0)
    tail_row = lax.broadcasted_iota(jnp.int32, (128, PIECE_ROWS), 1)
    for h in range(2):
        unstack = onehot(tail_row == last_row // 4 * PIECE + h * 4 + last_row % 4)
        for m in range(NCH // 2):
            at = h * (D // 2) + m * COLS
            tail = xel[:, :, m * COLS : (m + 1) * COLS].reshape(PIECE_ROWS, COLS)
            xl[:, at : at + COLS] = mm(unstack, tail).astype(BF16)
    hidl[...] = hidden(xl[...])

    for d in NEAR_FIRST[4:]:
        relay(d, zd, fd, rz_d, rp_d)

    wait_bytes(fd.at[:, pl.ds(0, INPLANE - 1)], rp_d)
    for h in range(2):
        for s in range(4):
            for px in range(4):
                for place in range(8):
                    col = h * 8 + place
                    dn[(s * 4 + px) * 16 : (s * 4 + px + 1) * 16, col * 128 : (col + 1) * 128] = fd[
                        h * 4 + s, px * 8 + place
                    ]
    piece_row = lax.broadcasted_iota(jnp.int32, (PIECE_ROWS, 128), 0)
    last_of = lax.broadcasted_iota(jnp.int32, (PIECE_ROWS, 128), 1)
    first = hid[...]
    last = mm(onehot(last_of == piece_row // PIECE * 4 + piece_row % 4), hidl[...]).astype(BF16)

    def send_piece(k, result):
        r[k] = result.astype(BF16).reshape(INPLANE, PIECE, COLS)

        @pl.loop(1, INPLANE)
        def _(j):
            place, device = hop(j)
            remote(r.at[k, place], rr.at[k, me], send_p, rp_r.at[k], device)

        rr[k, me] = r[k, me]

    for m in range(2):
        even, odd = (dn[:, n * COLS : (n + 1) * COLS] for n in (2 * m, 2 * m + 1))
        send_piece(2 * m, mm(first, even))
        send_piece(NCH + m, jnp.where(lower, mm(last, even), mm(last, odd)))
        send_piece(2 * m + 1, mm(first, odd))

    slot_row = lax.broadcasted_iota(jnp.int32, (SLOTS, PIECE_ROWS), 0)
    from_row = lax.broadcasted_iota(jnp.int32, (SLOTS, PIECE_ROWS), 1)
    back = onehot(placed(from_row // PIECE, from_row % PIECE) == slot_row)
    is_last = placed(from_row // PIECE, PIECE + from_row % 4) == slot_row
    back_last = [onehot(is_last & (from_row % PIECE // 4 == h)) for h in range(2)]
    for n in range(NCH):
        wait_bytes(rr.at[n, pl.ds(0, INPLANE - 1)], rp_r.at[n])
        tail = NCH + n // 2
        if n % 2 == 0:
            wait_bytes(rr.at[tail, pl.ds(0, INPLANE - 1)], rp_r.at[tail])
        moved = mm(back, rr[n].reshape(PIECE_ROWS, COLS)) + mm(back_last[n % 2], rr[tail].reshape(PIECE_ROWS, COLS))
        q[n] = moved.astype(BF16).reshape(GROUPS, GROUP_ROWS, COLS)
        for block in (3, 1, 2):
            remote(q.at[n, block], t.at[n, block], send_z, rz_r.at[n], z_device(row_sources[block]))

        t[n, 0] = q[n, 0]

    down_copy = pltpu.make_async_copy(dn, down_out.at[0], out_sem.at[2])
    down_copy.start()
    for h in range(2):
        for s in range(16):
            rows, cols = slice(h * 128, (h + 1) * 128), slice(s * 128, (s + 1) * 128)
            go[cols, rows] = gt[rows, cols].T
            uo[cols, rows] = ut[rows, cols].T
    gate_copy = pltpu.make_async_copy(go, gate_out.at[0], out_sem.at[0])
    up_copy = pltpu.make_async_copy(uo, up_out.at[0], out_sem.at[1])
    gate_copy.start()
    up_copy.start()

    select = [p.T.astype(BF16) for p in pick]
    weights = [jnp.broadcast_to(weight[k : k + 1, :], (128, TOK)).T[:, 0:1] for k in range(2)]
    for n in range(NCH):
        cols = slice(n * COLS, (n + 1) * COLS)
        wait_bytes(t.at[n, pl.ds(1, GROUPS - 1)], rz_r.at[n])
        table = t[n].reshape(SLOTS, COLS)
        mix[:, cols] = (mm(select[0], table) * weights[0] + mm(select[1], table) * weights[1]).astype(BF16)
    mixed_copy = pltpu.make_async_copy(mix, mixed_out, out_sem.at[3])
    mixed_copy.start()

    others = pl.ds(0, PLANES - 1)
    wait_bytes(zgu.at[others], send_z)
    wait_bytes(zd.at[others], send_z)
    wait_bytes(xz.at[pl.ds(0, GROUPS - 1)], send_z)
    wait_bytes(fgu.at[:, pl.ds(0, INPLANE - 1)], send_p)
    wait_bytes(fd.at[:, pl.ds(0, INPLANE - 1)], send_p)
    wait_bytes(xe.at[pl.ds(0, INPLANE - 1)], send_p)
    wait_bytes(xel.at[pl.ds(0, INPLANE - 1)], send_p)
    for n in range(NCH):
        wait_bytes(t.at[n, pl.ds(0, GROUPS - 1)], send_z)
    for k in range(PIECES):
        wait_bytes(rr.at[k, pl.ds(0, INPLANE - 1)], send_p)
    down_copy.wait()
    gate_copy.wait()
    up_copy.wait()
    mixed_copy.wait()


def write_out(*refs):
    srcs, dsts, bufs, in_sem, out_sem = refs[0:4], refs[4:8], refs[8:12], refs[12], refs[13]
    pieces = []
    for i in range(4):
        rows = srcs[i].shape[-2] // 2
        for h in range(2):
            cut = (0,) * (len(srcs[i].shape) - 2) + (pl.ds(h * rows, rows),)
            n = 2 * i + h
            pieces.append((
                pltpu.make_async_copy(srcs[i].at[cut], bufs[i].at[cut], in_sem.at[n]),
                pltpu.make_async_copy(bufs[i].at[cut], dsts[i].at[cut], out_sem.at[n]),
            ))
    for load, _ in pieces:
        load.start()
    for load, store in pieces:
        load.wait()
        store.start()
    for _, store in pieces:
        store.wait()


def body(
    tokens, norm_gain, gate_master, up_master, down_master, route_group, route_expert, route_weight
):
    vmem, hbm = pl.BlockSpec(memory_space=pltpu.VMEM), pl.BlockSpec(memory_space=pltpu.HBM)
    dma = pltpu.SemaphoreType.DMA
    tile = pltpu.VMEM
    shapes = (
        jax.ShapeDtypeStruct((1, D, F), BF16),
        jax.ShapeDtypeStruct((1, D, F), BF16),
        jax.ShapeDtypeStruct((1, F, D), BF16),
        jax.ShapeDtypeStruct((TOK, D), BF16),
    )
    outs = pl.pallas_call(
        kernel,
        out_shape=shapes,
        in_specs=[hbm, hbm, hbm, vmem, hbm, vmem, vmem, vmem],
        out_specs=(hbm,) * 4,
        scratch_shapes=[
            tile((3, 128, 16, 128), F32),
            tile((128, 32, 128), BF16),
            tile((128, 16, 128), BF16),
            tile((PLANES, INPLANE, 32, 128), BF16),
            tile((PLANES, INPLANE, 16, 128), BF16),
            tile((PLANES, INPLANE, 32, 128), BF16),
            tile((PLANES, INPLANE, 16, 128), BF16),
            tile((TOK, D), BF16),
            tile((GROUPS, GROUP_ROWS, D), BF16),
            tile((GROUPS, GROUP_ROWS, D), BF16),
            tile((INPLANE, PIECE, D), BF16),
            tile((INPLANE, PIECE, D // 2), BF16),
            tile((INPLANE, PIECE, D), BF16),
            tile((INPLANE, PIECE, D // 2), BF16),
            tile((128, D), BF16),
            tile((PIECE_ROWS, F), BF16),
            tile((128, F), BF16),
            tile((F, D), BF16),
            tile((F, D), BF16),
            tile((F, D), BF16),
            tile((D, F), BF16),
            tile((D, F), BF16),
            tile((PIECES, INPLANE, PIECE, COLS), BF16),
            tile((PIECES, INPLANE, PIECE, COLS), BF16),
            tile((NCH, GROUPS, GROUP_ROWS, COLS), BF16),
            tile((NCH, GROUPS, GROUP_ROWS, COLS), BF16),
            tile((TOK, D), BF16),
            dma((4,)),
            dma((4,)),
            dma,
            dma,
            dma((PLANES,)),
            dma((PLANES,)),
            dma,
            dma((NCH,)),
            dma,
            dma,
            dma((2,)),
            dma((PIECES,)),
        ],
        compiler_params=pltpu.CompilerParams(
            collective_id=0, has_side_effects=True, vmem_limit_bytes=60 * 2**20
        ),
    )(
        jnp.swapaxes(gate_master, 1, 2),
        jnp.swapaxes(up_master, 1, 2),
        down_master,
        norm_gain[None],
        tokens,
        route_group[None],
        route_expert.T,
        route_weight.T,
    )
    return pl.pallas_call(
        write_out,
        out_shape=shapes,
        in_specs=[hbm] * 4,
        out_specs=(hbm,) * 4,
        scratch_shapes=[tile(a.shape, a.dtype) for a in shapes] + [dma((8,)), dma((8,))],
        compiler_params=pltpu.CompilerParams(vmem_limit_bytes=60 * 2**20),
    )(*outs)


def solution(mesh):
    placed = (
        P(("gr", "fs", "tp"), None),
        P("fs"),
        P(None, "fs", ("gr", "tp")),
        P(None, "fs", ("gr", "tp")),
        P(None, "fs", ("gr", "tp")),
        P(("gr", "fs", "tp")),
        P(("gr", "fs", "tp"), None),
        P(("gr", "fs", "tp"), None),
    )
    return jax.shard_map(
        body,
        mesh=mesh,
        in_specs=placed,
        out_specs=(
            P(("fs", "tp"), None, None),
            P(("fs", "tp"), None, None),
            P(("fs", "tp"), None, None),
            P(("gr", "fs", "tp"), None),
        ),
        check_vma=False,
    )
```

```python
import functools

import jax
import jax.numpy as jnp
from jax import lax
from jax.experimental import pallas as pl
from jax.experimental.pallas import tpu as pltpu
from jax.sharding import PartitionSpec as P

MESH = pl.DeviceIdType.MESH
BF16 = jnp.bfloat16
F32 = jnp.float32

PLANES, GROUPS, INPLANE = 8, 4, 32
TOK, D, F, CAP = 128, 2048, 256, 3
GROUP_ROWS = INPLANE * CAP
SLOTS = GROUPS * GROUP_ROWS
NCH = 4
PIECE = 8
PIECE_ROWS = INPLANE * PIECE
PIECES = NCH + NCH // 2
COLS = D // NCH
NEAR_FIRST = (1, 7, 2, 6, 3, 5, 4)


def nt_dot(a, b):
    return lax.dot_general(a, b, (((1,), (1,)), ((), ())), preferred_element_type=F32)


def mm(a, b):
    return jnp.dot(a, b, preferred_element_type=F32)


def kernel(
    gate_in, up_in, down_in, gain, tok_in, group, expert, weight,
    gate_out, up_out, down_out, mixed_out,
    fbuf, wgu, wd, zgu, zd, fgu, fd,
    tokv, xzs, xz, xp, xpl, xe, xel, xl, hid, hidl,
    gt, ut, dn, go, uo, r, rr, q, t, mix,
    in_sem, out_sem, send_z, send_p, rz_gu, rz_d, rz_t, rz_r, rp_gu, rp_d, rp_t, rp_r,
):
    gr, fs, tp = lax.axis_index("gr"), lax.axis_index("fs"), lax.axis_index("tp")
    zl, x = lax.div(fs, 4), lax.rem(fs, 4)
    y, c = lax.div(tp, 2), lax.rem(tp, 2)
    z = gr * 4 + zl
    me = x * 8 + tp

    row_planes = [z] + [lax.rem(z + step, PLANES) for step in (1, 7, 2 + 4 * c)]
    row_sources = [z] + [lax.rem(z + step, PLANES) for step in (7, 1, 6 - 4 * c)]

    def z_device(target):
        return (lax.div(target, 4), lax.rem(target, 4) * 4 + x, tp)

    def hop(j):
        o = lax.rem(j * 21, INPLANE)
        tx = lax.rem(x + lax.div(o, 8), 4)
        ty = lax.rem(y + lax.rem(lax.div(o, 2), 4), 4)
        ttp = ty * 2 + lax.rem(c + lax.rem(o, 2), 2)
        return tx * 8 + ttp, (gr, zl * 4 + tx, ttp)

    def remote(src, dst, send, recv, device):
        pltpu.make_async_remote_copy(
            src_ref=src, dst_ref=dst, send_sem=send, recv_sem=recv, device_id=device, device_id_type=MESH
        ).start()

    def wait_bytes(ref, sem):
        pltpu.make_async_copy(ref, ref, sem).wait()

    barrier = pltpu.get_barrier_semaphore()
    for d in NEAR_FIRST:
        pl.semaphore_signal(barrier, inc=1, device_id=z_device(lax.rem(z + d, PLANES)), device_id_type=MESH)

    @pl.loop(1, INPLANE)
    def _(j):
        pl.semaphore_signal(barrier, inc=1, device_id=hop(j)[1], device_id_type=MESH)

    inputs = [
        pltpu.make_async_copy(src, dst, in_sem.at[i])
        for i, (src, dst) in enumerate(
            ((gate_in, fbuf.at[0]), (up_in, fbuf.at[1]), (down_in, fbuf.at[2]), (tok_in, tokv))
        )
    ]
    for copy in inputs:
        copy.start()
    inputs[3].wait()

    @pl.loop(0, 4)
    def _(i):
        rows = pl.ds(i * 32, 32)
        v = tokv[rows, :].astype(F32)
        v = v * lax.rsqrt(jnp.mean(v * v, axis=-1, keepdims=True) + 1e-06)
        tokv[rows, :] = v.astype(BF16)

    ids = group[...] * INPLANE + expert[...]
    expert_iota = lax.broadcasted_iota(jnp.int32, (128, TOK), 0)
    one = [(expert_iota == ids[k : k + 1, :]).astype(F32) for k in range(2)]
    lane_iota = lax.broadcasted_iota(jnp.int32, (128, TOK), 1)
    earlier = (expert_iota < lane_iota).astype(BF16)
    count = mm((one[0] + one[1]).astype(BF16), earlier)
    slot_iota = lax.broadcasted_iota(jnp.int32, (SLOTS, TOK), 0)
    away = lax.rem(group[...] - zl + GROUPS, GROUPS)
    block = jnp.where(away == 2, 3, jnp.where(away == 3, 2, away))
    pick = []
    for k in range(2):
        rank = jnp.sum(one[k] * count, axis=0, keepdims=True).astype(jnp.int32)
        slot = jnp.where(rank < CAP, block * GROUP_ROWS + expert[k : k + 1, :] * CAP + rank, -1)
        pick.append((slot_iota == slot).astype(F32))
    rows_of = (pick[0] + pick[1]).astype(BF16)
    for n in range(NCH):
        cols = slice(n * COLS, (n + 1) * COLS)
        xzs[:, :, cols] = mm(rows_of, tokv[:, cols]).astype(BF16).reshape(GROUPS, GROUP_ROWS, COLS)
    inputs[0].wait()
    inputs[1].wait()
    scale = gain[...].reshape(1, 1, 128)

    @pl.loop(0, 16)
    def _(i):
        e = pl.ds(i * 8, 8)
        wgu[e, 0:16, :] = (fbuf[0, e] * scale).astype(BF16)
        wgu[e, 16:32, :] = (fbuf[1, e] * scale).astype(BF16)

    inputs[2].wait()

    @pl.loop(0, 16)
    def _(i):
        e = pl.ds(i * 8, 8)
        wd[e] = fbuf[2, e].astype(BF16)

    pl.semaphore_wait(barrier, len(NEAR_FIRST) + INPLANE - 1)

    def send_planes(src, dst, recv, steps):
        for d in steps:
            target = lax.rem(z + d, PLANES)
            experts = pl.ds(lax.rem(target, 4) * INPLANE, INPLANE)
            remote(src.at[experts], dst.at[z], send_z, recv.at[z], z_device(target))

    def forward(src, base, dst, plane, recv):
        @pl.loop(1, INPLANE)
        def _(j):
            place, device = hop(j)
            remote(src.at[base + place], dst.at[plane, me], send_p, recv, device)

    for block in (3, 1, 2):
        remote(xzs.at[block], xz.at[block], send_z, rz_t, z_device(row_planes[block]))

    send_planes(wgu, zgu, rz_gu, NEAR_FIRST)
    send_planes(wd, zd, rz_d, NEAR_FIRST)
    forward(wgu, zl * INPLANE, fgu, z, rp_gu)
    forward(wd, zl * INPLANE, fd, z, rp_d)
    fgu[z, me] = wgu[zl * INPLANE + me]
    fd[z, me] = wd[zl * INPLANE + me]

    @pl.loop(0, GROUP_ROWS // 16)
    def _(i):
        rows = pl.ds(i * 16, 16)
        xz[0, rows, :] = xzs[0, rows, :]

    def relay(d, src, dst, rz, rp):
        plane = lax.rem(z + PLANES - d, PLANES)
        wait_bytes(src.at[plane], rz.at[plane])

        @pl.loop(1, INPLANE)
        def _(j):
            place, device = hop(j)
            remote(src.at[plane, place], dst.at[plane, me], send_p, rp, device)

        dst[plane, me] = src[plane, me]

    def placed(place, within):
        block = (within >= 3).astype(jnp.int32) + (within >= 6).astype(jnp.int32) + (within >= 9).astype(jnp.int32)
        at = block * GROUP_ROWS + place * CAP + within - block * CAP
        return jnp.where(within < GROUPS * CAP, at, -1)

    def onehot(mask):
        return mask.astype(F32).astype(BF16)

    wait_bytes(xz.at[pl.ds(1, GROUPS - 1)], rz_t)
    to = lax.broadcasted_iota(jnp.int32, (PIECE_ROWS, SLOTS), 0)
    of = lax.broadcasted_iota(jnp.int32, (PIECE_ROWS, SLOTS), 1)
    order = onehot(placed(to // PIECE, to % PIECE) == of)
    order_last = onehot(placed(to // PIECE, PIECE + to % 4) == of)
    lower = lax.broadcasted_iota(jnp.int32, (PIECE_ROWS, COLS), 0) % PIECE < 4
    halves = []
    for n in range(NCH):
        cols = slice(n * COLS, (n + 1) * COLS)
        rows = xz[:, :, cols].reshape(SLOTS, COLS)
        xp[:, :, cols] = mm(order, rows).astype(BF16).reshape(INPLANE, PIECE, COLS)
        halves.append(mm(order_last, rows))
    for m in range(NCH // 2):
        both = jnp.where(lower, halves[m], halves[m + NCH // 2])
        xpl[:, :, m * COLS : (m + 1) * COLS] = both.astype(BF16).reshape(INPLANE, PIECE, COLS)

    @pl.loop(1, INPLANE)
    def _(j):
        place, device = hop(j)
        remote(xp.at[place], xe.at[me], send_p, rp_t.at[0], device)
        remote(xpl.at[place], xel.at[me], send_p, rp_t.at[1], device)

    xe[me] = xp[me]
    xel[me] = xpl[me]

    for d in NEAR_FIRST:
        relay(d, zgu, fgu, rz_gu, rp_gu)

    for d in NEAR_FIRST[:4]:
        relay(d, zd, fd, rz_d, rp_d)

    wait_bytes(fgu.at[:, pl.ds(0, INPLANE - 1)], rp_gu)
    for h in range(2):
        for s in range(4):
            for px in range(4):
                rows, cols = slice(h * 128, (h + 1) * 128), slice((s * 4 + px) * 128, (s * 4 + px + 1) * 128)
                tiles = slice(px * 8, (px + 1) * 8)
                gt[rows, cols] = fgu[h * 4 + s, tiles, 0:16, :].reshape(128, 128)
                ut[rows, cols] = fgu[h * 4 + s, tiles, 16:32, :].reshape(128, 128)
    wait_bytes(xe.at[pl.ds(0, INPLANE - 1)], rp_t.at[0])
    wait_bytes(xel.at[pl.ds(0, INPLANE - 1)], rp_t.at[1])

    def hidden(rows):
        gate = nt_dot(rows, gt[...])
        upper = nt_dot(rows, ut[...])
        return (gate / (1.0 + jnp.exp(-gate)) * upper).astype(BF16)

    @pl.loop(0, PIECE_ROWS // 128)
    def _(i):
        hid[pl.ds(i * 128, 128), :] = hidden(xe[pl.ds(i * 16, 16)].reshape(128, D))

    last_row = lax.broadcasted_iota(jnp.int32, (128, PIECE_ROWS), 0)
    tail_row = lax.broadcasted_iota(jnp.int32, (128, PIECE_ROWS), 1)
    for h in range(2):
        unstack = onehot(tail_row == last_row // 4 * PIECE + h * 4 + last_row % 4)
        for m in range(NCH // 2):
            at = h * (D // 2) + m * COLS
            tail = xel[:, :, m * COLS : (m + 1) * COLS].reshape(PIECE_ROWS, COLS)
            xl[:, at : at + COLS] = mm(unstack, tail).astype(BF16)
    hidl[...] = hidden(xl[...])

    for d in NEAR_FIRST[4:]:
        relay(d, zd, fd, rz_d, rp_d)

    wait_bytes(fd.at[:, pl.ds(0, INPLANE - 1)], rp_d)
    for h in range(2):
        for s in range(4):
            for px in range(4):
                for place in range(8):
                    col = h * 8 + place
                    dn[(s * 4 + px) * 16 : (s * 4 + px + 1) * 16, col * 128 : (col + 1) * 128] = fd[
                        h * 4 + s, px * 8 + place
                    ]
    piece_row = lax.broadcasted_iota(jnp.int32, (PIECE_ROWS, 128), 0)
    last_of = lax.broadcasted_iota(jnp.int32, (PIECE_ROWS, 128), 1)
    first = hid[...]
    last = mm(onehot(last_of == piece_row // PIECE * 4 + piece_row % 4), hidl[...]).astype(BF16)

    def send_piece(k, result):
        r[k] = result.astype(BF16).reshape(INPLANE, PIECE, COLS)

        @pl.loop(1, INPLANE)
        def _(j):
            place, device = hop(j)
            remote(r.at[k, place], rr.at[k, me], send_p, rp_r.at[k], device)

        rr[k, me] = r[k, me]

    for m in range(2):
        even, odd = (dn[:, n * COLS : (n + 1) * COLS] for n in (2 * m, 2 * m + 1))
        send_piece(2 * m, mm(first, even))
        send_piece(NCH + m, jnp.where(lower, mm(last, even), mm(last, odd)))
        send_piece(2 * m + 1, mm(first, odd))

    slot_row = lax.broadcasted_iota(jnp.int32, (SLOTS, PIECE_ROWS), 0)
    from_row = lax.broadcasted_iota(jnp.int32, (SLOTS, PIECE_ROWS), 1)
    back = onehot(placed(from_row // PIECE, from_row % PIECE) == slot_row)
    is_last = placed(from_row // PIECE, PIECE + from_row % 4) == slot_row
    back_last = [onehot(is_last & (from_row % PIECE // 4 == h)) for h in range(2)]
    for n in range(NCH):
        wait_bytes(rr.at[n, pl.ds(0, INPLANE - 1)], rp_r.at[n])
        tail = NCH + n // 2
        if n % 2 == 0:
            wait_bytes(rr.at[tail, pl.ds(0, INPLANE - 1)], rp_r.at[tail])
        moved = mm(back, rr[n].reshape(PIECE_ROWS, COLS)) + mm(back_last[n % 2], rr[tail].reshape(PIECE_ROWS, COLS))
        q[n] = moved.astype(BF16).reshape(GROUPS, GROUP_ROWS, COLS)
        for block in (3, 1, 2):
            remote(q.at[n, block], t.at[n, block], send_z, rz_r.at[n], z_device(row_sources[block]))

        t[n, 0] = q[n, 0]

    down_copy = pltpu.make_async_copy(dn, down_out.at[0], out_sem.at[2])
    down_copy.start()
    for h in range(2):
        for s in range(16):
            rows, cols = slice(h * 128, (h + 1) * 128), slice(s * 128, (s + 1) * 128)
            go[cols, rows] = gt[rows, cols].T
            uo[cols, rows] = ut[rows, cols].T
    gate_copy = pltpu.make_async_copy(go, gate_out.at[0], out_sem.at[0])
    up_copy = pltpu.make_async_copy(uo, up_out.at[0], out_sem.at[1])
    gate_copy.start()
    up_copy.start()

    select = [p.T.astype(BF16) for p in pick]
    weights = [jnp.broadcast_to(weight[k : k + 1, :], (128, TOK)).T[:, 0:1] for k in range(2)]
    for n in range(NCH):
        cols = slice(n * COLS, (n + 1) * COLS)
        wait_bytes(t.at[n, pl.ds(1, GROUPS - 1)], rz_r.at[n])
        table = t[n].reshape(SLOTS, COLS)
        mix[:, cols] = (mm(select[0], table) * weights[0] + mm(select[1], table) * weights[1]).astype(BF16)
    mixed_copy = pltpu.make_async_copy(mix, mixed_out, out_sem.at[3])
    mixed_copy.start()

    others = pl.ds(0, PLANES - 1)
    wait_bytes(zgu.at[others], send_z)
    wait_bytes(zd.at[others], send_z)
    wait_bytes(xz.at[pl.ds(0, GROUPS - 1)], send_z)
    wait_bytes(fgu.at[:, pl.ds(0, INPLANE - 1)], send_p)
    wait_bytes(fd.at[:, pl.ds(0, INPLANE - 1)], send_p)
    wait_bytes(xe.at[pl.ds(0, INPLANE - 1)], send_p)
    wait_bytes(xel.at[pl.ds(0, INPLANE - 1)], send_p)
    for n in range(NCH):
        wait_bytes(t.at[n, pl.ds(0, GROUPS - 1)], send_z)
    for k in range(PIECES):
        wait_bytes(rr.at[k, pl.ds(0, INPLANE - 1)], send_p)
    down_copy.wait()
    gate_copy.wait()
    up_copy.wait()
    mixed_copy.wait()


def write_out(*refs):
    srcs, dsts, bufs, in_sem, out_sem = refs[0:4], refs[4:8], refs[8:12], refs[12], refs[13]
    pieces = []
    for i in range(4):
        rows = srcs[i].shape[-2] // 4
        for h in range(4):
            cut = (0,) * (len(srcs[i].shape) - 2) + (pl.ds(h * rows, rows),)
            n = 4 * i + h
            pieces.append((
                pltpu.make_async_copy(srcs[i].at[cut], bufs[i].at[cut], in_sem.at[n]),
                pltpu.make_async_copy(bufs[i].at[cut], dsts[i].at[cut], out_sem.at[n]),
            ))
    for load, _ in pieces:
        load.start()
    for load, store in pieces:
        load.wait()
        store.start()
    for _, store in pieces:
        store.wait()


def body(
    tokens, norm_gain, gate_master, up_master, down_master, route_group, route_expert, route_weight
):
    vmem, hbm = pl.BlockSpec(memory_space=pltpu.VMEM), pl.BlockSpec(memory_space=pltpu.HBM)
    dma = pltpu.SemaphoreType.DMA
    tile = pltpu.VMEM
    shapes = (
        jax.ShapeDtypeStruct((1, D, F), BF16),
        jax.ShapeDtypeStruct((1, D, F), BF16),
        jax.ShapeDtypeStruct((1, F, D), BF16),
        jax.ShapeDtypeStruct((TOK, D), BF16),
    )
    outs = pl.pallas_call(
        kernel,
        out_shape=shapes,
        in_specs=[hbm, hbm, hbm, vmem, hbm, vmem, vmem, vmem],
        out_specs=(hbm,) * 4,
        scratch_shapes=[
            tile((3, 128, 16, 128), F32),
            tile((128, 32, 128), BF16),
            tile((128, 16, 128), BF16),
            tile((PLANES, INPLANE, 32, 128), BF16),
            tile((PLANES, INPLANE, 16, 128), BF16),
            tile((PLANES, INPLANE, 32, 128), BF16),
            tile((PLANES, INPLANE, 16, 128), BF16),
            tile((TOK, D), BF16),
            tile((GROUPS, GROUP_ROWS, D), BF16),
            tile((GROUPS, GROUP_ROWS, D), BF16),
            tile((INPLANE, PIECE, D), BF16),
            tile((INPLANE, PIECE, D // 2), BF16),
            tile((INPLANE, PIECE, D), BF16),
            tile((INPLANE, PIECE, D // 2), BF16),
            tile((128, D), BF16),
            tile((PIECE_ROWS, F), BF16),
            tile((128, F), BF16),
            tile((F, D), BF16),
            tile((F, D), BF16),
            tile((F, D), BF16),
            tile((D, F), BF16),
            tile((D, F), BF16),
            tile((PIECES, INPLANE, PIECE, COLS), BF16),
            tile((PIECES, INPLANE, PIECE, COLS), BF16),
            tile((NCH, GROUPS, GROUP_ROWS, COLS), BF16),
            tile((NCH, GROUPS, GROUP_ROWS, COLS), BF16),
            tile((TOK, D), BF16),
            dma((4,)),
            dma((4,)),
            dma,
            dma,
            dma((PLANES,)),
            dma((PLANES,)),
            dma,
            dma((NCH,)),
            dma,
            dma,
            dma((2,)),
            dma((PIECES,)),
        ],
        compiler_params=pltpu.CompilerParams(
            collective_id=0, has_side_effects=True, vmem_limit_bytes=60 * 2**20
        ),
    )(
        jnp.swapaxes(gate_master, 1, 2),
        jnp.swapaxes(up_master, 1, 2),
        down_master,
        norm_gain[None],
        tokens,
        route_group[None],
        route_expert.T,
        route_weight.T,
    )
    return pl.pallas_call(
        write_out,
        out_shape=shapes,
        in_specs=[hbm] * 4,
        out_specs=(hbm,) * 4,
        scratch_shapes=[tile(a.shape, a.dtype) for a in shapes] + [dma((16,)), dma((16,))],
        compiler_params=pltpu.CompilerParams(vmem_limit_bytes=60 * 2**20),
    )(*outs)


def solution(mesh):
    placed = (
        P(("gr", "fs", "tp"), None),
        P("fs"),
        P(None, "fs", ("gr", "tp")),
        P(None, "fs", ("gr", "tp")),
        P(None, "fs", ("gr", "tp")),
        P(("gr", "fs", "tp")),
        P(("gr", "fs", "tp"), None),
        P(("gr", "fs", "tp"), None),
    )
    return jax.shard_map(
        body,
        mesh=mesh,
        in_specs=placed,
        out_specs=(
            P(("fs", "tp"), None, None),
            P(("fs", "tp"), None, None),
            P(("fs", "tp"), None, None),
            P(("gr", "fs", "tp"), None),
        ),
        check_vma=False,
    )
```
